256 devices in a mesh: dp: 4 (over y), kv: 32 (over z, x), tp: 2 (over core).
Axes of the slice: x: 4, y: 4, z: 8, core: 2. Of those that a mesh axis runs over, the one named last changes fastest.
Arguments:
- tokens: bfloat16 [16, 16, 2048], P('dp', None, 'kv'), may hold values from -6 to 6
- norm_gain: float32 [2048], P('kv'), may hold values from 0.1 to 1.9
- w_query: bfloat16 [2048, 1024], P('kv', 'tp'), may hold values from -0.125 to 0.125
- w_key: bfloat16 [2048, 1024], P('kv', 'tp'), may hold values from -0.125 to 0.125
- w_value: bfloat16 [2048, 1024], P('kv', 'tp'), may hold values from -0.125 to 0.125
- w_forget: bfloat16 [2048, 16], replicated, may hold values from -0.125 to 0.125
- forget_bias: float32 [16], replicated, may hold values from -2 to 4
- query_gain: float32 [64], replicated, may hold values from 0.1 to 1.9
- key_gain: float32 [64], replicated, may hold values from 0.1 to 1.9
- head_gain: float32 [64], replicated, may hold values from 0.1 to 1.9
- w_out: bfloat16 [1024, 2048], P('tp', 'kv'), may hold values from -0.1875 to 0.1875
- key_cache: bfloat16 [16, 16384, 1024], P('dp', 'kv', 'tp'), may hold values from -240 to 240
- value_cache: bfloat16 [16, 16384, 1024], P('dp', 'kv', 'tp'), may hold values from -6 to 6
- gate_cache: float32 [16, 16, 16384], P('dp', 'tp', 'kv'), may hold values from -1922 to 0, as said below
- lengths: int32 [16], P('dp'), may hold values from 15341 to 16364
- accepted: int32 [16], P('dp'), may hold values from 0 to 4
- parents: int32 [16, 16], P('dp'), may hold values from -1 to 14, as said below
Outputs:
- layer_out: bfloat16 [16, 16, 2048], P('dp', None, 'kv')
- new_keys: bfloat16 [16, 16384, 1024], P('dp', 'kv', 'tp')
- new_values: bfloat16 [16, 16384, 1024], P('dp', 'kv', 'tp')
- proposal_gates: float32 [16, 16, 16], P('dp', None, 'tp')
The draws below stay inside these ranges and needn't reach their ends.
Inputs may be any that keep to these rules, and one draw needn't show every extreme that they name: `gate_cache`: each entry is the running sum of log forget gates up to its position, so entries never rise along positions; entries at and after lengths hold the last step's proposals in order. `parents`: proposal 0 follows the last accepted token (parent -1); every other proposal's parent is one of the three proposals before it.
All inputs are finite; a program needn't handle non-finite values.
Results may differ from the reference program's by a relative error of at most 0.0051.
The reference program's roundings to bfloat16 on the way (of `scaled`, `values_new` and `normed`) count: a program that leaves them out, or rounds other values in their place, can miss the bound.
Values may be sent and summed in bfloat16 or wider, within the bound.
No kernel may reach another device: no remote copies, remote signals or barrier semaphores. Data moves between devices by JAX's collectives and lax.ppermute only.
A program may use at most 64 MiB of HBM per device.

```python
import jax
import jax.numpy as jnp
from jax import lax

D = 2048
HEADS = 16
DH = 64
PROPS = 16
ACCEPT_MOST = 4
POS_DEV = 512
HW = 1024
HEAD_GROUP = 8
SEQUENCE_TOTAL = 16
CACHE_POSITIONS = 16384
N_KV = 32
N_TP = 2


def draw_key_cache(key, part):
    key_one = jax.random.fold_in(key, 0)
    entries = jnp.clip(jax.random.normal(key_one, (SEQUENCE_TOTAL, CACHE_POSITIONS, HEADS * DH), jnp.float32), -6.0, 6.0)
    return entries.astype(jnp.bfloat16)


def draw_gate_cache(key, part):
    every_key = jax.random.split(key, 7)
    slow_share = 0.5
    slow_heads = jax.random.uniform(every_key[0], (SEQUENCE_TOTAL, HEADS, 1)) < slow_share
    slow_rate = jax.random.uniform(every_key[1], (SEQUENCE_TOTAL, HEADS, 1), minval=0.2, maxval=0.8) / CACHE_POSITIONS
    fast_rate = 1.0 / (POS_DEV * jax.random.uniform(every_key[2], (SEQUENCE_TOTAL, HEADS, 1), minval=0.06, maxval=0.2))
    decay_rates = jnp.where(slow_heads, slow_rate, fast_rate)
    block_multiplier = jnp.exp(jax.random.uniform(every_key[3], (SEQUENCE_TOTAL, HEADS, CACHE_POSITIONS // POS_DEV), minval=-0.7, maxval=0.7))
    block_multiplier = jnp.repeat(block_multiplier, POS_DEV, axis=2)
    coarse_estimate = jax.random.uniform(every_key[4], (SEQUENCE_TOTAL, HEADS, CACHE_POSITIONS), minval=0.3, maxval=1.7)
    flurry_position = jax.random.randint(every_key[5], (SEQUENCE_TOTAL, 1, 2), 0, CACHE_POSITIONS)
    position_numbers = jnp.arange(CACHE_POSITIONS, dtype=jnp.int32)[None, None, :]
    flurry_groups = ((position_numbers == flurry_position[..., 0:1]) | (position_numbers == flurry_position[..., 1:2])).astype(jnp.float32)
    tree_depth = jax.random.uniform(every_key[6], (SEQUENCE_TOTAL, HEADS, 1), minval=0.22, maxval=0.69)
    logarithm_gates = -decay_rates * block_multiplier * coarse_estimate - flurry_groups * tree_depth
    return jnp.cumsum(logarithm_gates, axis=2).astype(jnp.float32)


def draw_parents(key, part):
    draws = jax.random.randint(key, (SEQUENCE_TOTAL, PROPS), 0, 3, dtype=jnp.int32)
    step_ids = jnp.arange(PROPS, dtype=jnp.int32)[None, :]
    back_steps = draws % jnp.maximum(jnp.minimum(step_ids, 3), 1)
    return jnp.where(step_ids == 0, -1, step_ids - 1 - back_steps).astype(jnp.int32)


def with_ends(values, key, low, high):
    longest = values.shape.index(max(values.shape))
    spots = []
    for shift in (0, 1):
        where = [jax.random.randint(jax.random.fold_in(key, axis), (), 0, length) for axis, length in enumerate(values.shape)]
        where[longest] = (where[longest] + shift) % values.shape[longest]
        spots.append(tuple(where))
    return values.at[spots[0]].set(low).at[spots[1]].set(high)


def block_levels(rng, shape, cuts, low, top_value):
    level, own = 1.0, jax.random.fold_in(rng, 6)
    for axis_at, shards_of in cuts:
        heights = jnp.exp(jax.random.uniform(jax.random.fold_in(own, axis_at), (shards_of,), jnp.float32, low / len(cuts), top_value / len(cuts)))
        level = level * jnp.repeat(heights, shape[axis_at] // shards_of).reshape([-1 if axis == axis_at else 1 for axis in range(len(shape))])
    return level


def gaussian(key, dims, width, most, shards=(), kind=jnp.bfloat16):
    gain = block_levels(key, dims, shards, -0.22, 0.18) if shards else 1.0
    drawn = jax.random.normal(key, dims, jnp.float32) * width * gain
    return jnp.minimum(jnp.maximum(drawn, -most), most).astype(kind)


def setup_inputs(seed: int = 0) -> dict:
    arg_keys = jax.random.split(jax.random.key(seed), 18)
    tokens = gaussian(arg_keys[0], (SEQUENCE_TOTAL, PROPS, D), 1.0, 6.0, ((0, 4), (2, 32)))
    norm_gain = jnp.clip(1.0 + 0.18 * jax.random.normal(arg_keys[1], (D,), jnp.float32), 0.1, 1.9)
    w_query = gaussian(arg_keys[2], (D, HW), D ** -0.5, 0.125, ((0, 32), (1, 2)))
    w_key = gaussian(arg_keys[3], (D, HW), D ** -0.5, 0.125, ((0, 32), (1, 2)))
    w_value = gaussian(arg_keys[4], (D, HW), D ** -0.5, 0.125, ((0, 32), (1, 2)))
    w_forget = gaussian(arg_keys[5], (D, HEADS), D ** -0.5, 0.125)
    forget_bias = jnp.clip(jax.random.uniform(arg_keys[6], (HEADS,), jnp.float32, -2.0, 4.0), -2.0, 4.0)
    query_gain = jnp.clip(1.0 + 0.18 * jax.random.normal(arg_keys[7], (DH,), jnp.float32), 0.1, 1.9)
    key_gain = jnp.clip(1.0 + 0.18 * jax.random.normal(arg_keys[8], (DH,), jnp.float32), 0.1, 1.9)
    head_gain = jnp.clip(1.0 + 0.18 * jax.random.normal(arg_keys[9], (DH,), jnp.float32), 0.1, 1.9)
    w_out = gaussian(arg_keys[10], (HW, D), HW ** -0.5, 0.1875, ((0, 2), (1, 32)))
    key_cache = draw_key_cache(jax.random.fold_in(arg_keys[17], 71), 0)
    value_cache = gaussian(arg_keys[12], (SEQUENCE_TOTAL, CACHE_POSITIONS, HW), 1.0, 6.0, ((0, 4), (1, 32), (2, 2)))
    gate_cache = draw_gate_cache(jax.random.fold_in(arg_keys[17], 71), 0)
    lengths = with_ends(jax.random.randint(arg_keys[14], (SEQUENCE_TOTAL,), CACHE_POSITIONS - PROPS - ACCEPT_MOST + 1 - 2 * POS_DEV, CACHE_POSITIONS - PROPS - ACCEPT_MOST + 1), jax.random.fold_in(arg_keys[14], 1), CACHE_POSITIONS - PROPS - ACCEPT_MOST + 1 - 2 * POS_DEV, CACHE_POSITIONS - PROPS - ACCEPT_MOST).astype(jnp.int32)
    accepted = with_ends(jax.random.randint(arg_keys[15], (SEQUENCE_TOTAL,), 0, ACCEPT_MOST + 1), jax.random.fold_in(arg_keys[15], 1), 0, ACCEPT_MOST).astype(jnp.int32)
    parents = draw_parents(jax.random.fold_in(arg_keys[17], 71), 0)
    return dict(tokens=tokens, norm_gain=norm_gain, w_query=w_query, w_key=w_key, w_value=w_value, w_forget=w_forget, forget_bias=forget_bias, query_gain=query_gain, key_gain=key_gain, head_gain=head_gain, w_out=w_out, key_cache=key_cache, value_cache=value_cache, gate_cache=gate_cache, lengths=lengths, accepted=accepted, parents=parents)


EPSILON = 1e-06
MASKED = -1e+30

def head_norm(head_rows, gain_vec):
    mean_square = lax.optimization_barrier(jnp.mean(head_rows * head_rows, axis=-1, keepdims=True))
    return head_rows * lax.rsqrt(mean_square + EPSILON) * gain_vec

def ancestry(parents):
    count_all = parents.shape[0]
    step_ids = jnp.arange(count_all, dtype=jnp.int32)
    step_matrix = (parents[:, None] == step_ids[None, :]).astype(jnp.float32)
    identity = jnp.eye(count_all, dtype=jnp.float32)

    def extend(turn_index, ancestors):
        return identity + jnp.dot(step_matrix, ancestors, precision=lax.Precision.HIGHEST)
    return lax.fori_loop(0, count_all, extend, identity)

def softmax_block(scores, live_mask, block_values):
    row_max = lax.optimization_barrier(jnp.max(scores, axis=-1))
    weights = jnp.where(live_mask, jnp.exp(scores - row_max[..., None]), 0.0)
    row_total = lax.optimization_barrier(jnp.sum(weights, axis=-1))
    rounded = lax.optimization_barrier(weights.astype(jnp.bfloat16)).astype(jnp.float32)
    weighted = jnp.einsum('hpk,khd->phd', rounded, block_values.astype(jnp.float32))
    return (row_max.T, row_total.T, weighted)

def combine(earlier, later):
    earlier_max, earlier_total, earlier_sum = earlier
    later_max, later_total, later_sum = later
    row_max = jnp.maximum(earlier_max, later_max)
    earlier_scale = jnp.exp(earlier_max - row_max)
    later_scale = jnp.exp(later_max - row_max)
    return (row_max, earlier_total * earlier_scale + later_total * later_scale, earlier_sum * earlier_scale[..., None] + later_sum * later_scale[..., None])

def one_sequence(items, shared):
    tokens, key_cache, value_cache, gate_cache, length, accept, parents = items
    norm_gain, w_query, w_key, w_value, w_forget, forget_bias, query_gain, key_gain, head_gain, w_out = shared
    token_rows = tokens.astype(jnp.float32)
    inverse = lax.rsqrt(lax.optimization_barrier(jnp.mean(token_rows * token_rows, axis=1)) + EPSILON)[:, None]
    scaled = (token_rows * norm_gain).astype(jnp.bfloat16)
    query_raw = jnp.dot(scaled, w_query, preferred_element_type=jnp.float32) * inverse
    key_raw = jnp.dot(scaled, w_key, preferred_element_type=jnp.float32) * inverse
    value_raw = jnp.dot(scaled, w_value, preferred_element_type=jnp.float32) * inverse
    gate_raw = jnp.dot(scaled, w_forget, preferred_element_type=jnp.float32) * inverse
    queries = head_norm(query_raw.reshape(PROPS, HEADS, DH), query_gain).astype(jnp.bfloat16)
    keys_new = head_norm(key_raw.reshape(PROPS, HEADS, DH), key_gain).astype(jnp.bfloat16)
    values_new = value_raw.astype(jnp.bfloat16).reshape(PROPS, HEADS, DH)
    logarithm_gates = jax.nn.log_sigmoid(gate_raw + forget_bias)
    ancestors = ancestry(parents)
    path_sum = jnp.dot(ancestors, logarithm_gates, precision=lax.Precision.HIGHEST)
    base_pos = length + accept
    boundary = lax.dynamic_slice_in_dim(gate_cache, base_pos - 1, 1, 1)[:, 0]
    score_scale = DH ** (-0.5)
    score_shift = boundary[:, None, None] + path_sum.T[:, :, None]
    key_blocks = key_cache.reshape(N_KV, POS_DEV, HEADS, DH)
    value_blocks = value_cache.reshape(N_KV, POS_DEV, HEADS, DH)
    gate_blocks = gate_cache.reshape(HEADS, N_KV, POS_DEV).transpose(1, 0, 2)
    block_starts = jnp.arange(N_KV, dtype=jnp.int32) * POS_DEV
    query_wide = queries.astype(jnp.float32)

    def cache_block(block_args):
        block_keys, block_values, block_gates, block_start = block_args
        scores = jnp.einsum('phd,khd->hpk', query_wide, block_keys.astype(jnp.float32)) * score_scale
        scores = scores + score_shift - block_gates[:, None, :]
        live_mask = (block_start + jnp.arange(POS_DEV, dtype=jnp.int32) < base_pos)[None, None, :]
        scores = jnp.where(live_mask, scores, MASKED)
        return softmax_block(scores, live_mask, block_values)
    block_max, block_total, block_sum = lax.map(cache_block, (key_blocks, value_blocks, gate_blocks, block_starts))
    row_max = lax.optimization_barrier(jnp.max(block_max, axis=0))
    factors = jnp.exp(block_max - row_max)
    cache_part = (row_max, lax.optimization_barrier(jnp.sum(block_total * factors, axis=0)), lax.optimization_barrier(jnp.sum(block_sum * factors[..., None], axis=0)))
    tree_scores = jnp.einsum('phd,jhd->hpj', query_wide, keys_new.astype(jnp.float32)) * score_scale
    tree_scores = tree_scores + path_sum.T[:, :, None] - path_sum.T[:, None, :]
    tree_live = (ancestors > 0.5)[None]
    tree_scores = jnp.where(tree_live, tree_scores, MASKED)
    tree_part = softmax_block(tree_scores, tree_live, values_new)
    row_max, row_total, weighted = combine(cache_part, tree_part)
    attended = weighted / row_total[..., None]
    normed = head_norm(attended, head_gain).astype(jnp.bfloat16).reshape(PROPS, HW)
    group_width = HEAD_GROUP * DH
    layer_sum = jnp.zeros((PROPS, D), jnp.float32)
    for group_index in range(N_TP):
        lower = group_index * group_width
        group_term = jnp.dot(normed[:, lower:lower + group_width], w_out[lower:lower + group_width], preferred_element_type=jnp.float32)
        layer_sum = layer_sum + lax.optimization_barrier(group_term.astype(jnp.bfloat16)).astype(jnp.float32)
    layer_out = layer_sum.astype(jnp.bfloat16)
    zero_index = jnp.zeros((), jnp.int32)
    new_keys = lax.dynamic_update_slice(key_cache, keys_new.reshape(PROPS, HW), (base_pos, zero_index))
    new_values = lax.dynamic_update_slice(value_cache, values_new.reshape(PROPS, HW), (base_pos, zero_index))
    return (layer_out, new_keys, new_values, logarithm_gates)

def reference(tokens, norm_gain, w_query, w_key, w_value, w_forget, forget_bias, query_gain, key_gain, head_gain, w_out, key_cache, value_cache, gate_cache, lengths, accepted, parents):
    shared = (norm_gain, w_query, w_key, w_value, w_forget, forget_bias, query_gain, key_gain, head_gain, w_out)

    def per_sequence(items):
        return one_sequence(items, shared)
    layer_out, new_keys, new_values, proposal_gates = lax.map(per_sequence, (tokens, key_cache, value_cache, gate_cache, lengths, accepted, parents))
    return (layer_out, new_keys, new_values, proposal_gates)
```

```python
import jax
import jax.numpy as jnp
from jax import lax
from jax.experimental import pallas as pl
from jax.experimental.pallas import tpu as pltpu
from jax.sharding import PartitionSpec as P

EPSILON = 1e-06
MASKED = -1e30
F32 = jnp.float32
BF16 = jnp.bfloat16

LANES = 128
SUB = 8
N_KV = 32
GROUPS = 8
QUARTERS = 4
ROWS = 64
HEADS = 8
DH = 64
WIDTH = 512
PROPS = 16
SEQS = 4
BLOCK = 512
SEND_A = 26
SEND_B = 32
SEND_C = 16


def iota(shape, dim):
    return lax.broadcasted_iota(jnp.int32, shape, dim)


def dot_nn(a, b):
    return lax.dot_general(a, b, (((1,), (0,)), ((), ())), preferred_element_type=F32)


def dot_nt(a, b):
    return lax.dot_general(a, b, (((1,), (1,)), ((), ())), preferred_element_type=F32)


def pieces(x):
    high = x.astype(BF16).astype(F32)
    rest = x - high
    middle = rest.astype(BF16).astype(F32)
    return high, middle, rest - middle


def vmem():
    return pl.BlockSpec(memory_space=pltpu.VMEM)


def stay(array):
    return pltpu.with_memory_space_constraint(array, pltpu.HBM)


def close(array):
    return pltpu.with_memory_space_constraint(array, pltpu.VMEM)


def hbm():
    return pl.BlockSpec(memory_space=pltpu.HBM)


def smem():
    return pl.BlockSpec(memory_space=pltpu.SMEM)


def cost(flops, moved):
    return pl.CostEstimate(flops=flops, bytes_accessed=moved, transcendentals=0)


def doubled(gain_ref):
    gain = gain_ref[...]
    return jnp.concatenate([gain, gain], axis=1)


def project_kernel(
    x_hbm, gain_hbm, wq_hbm, wk_hbm, wv_hbm, wf_hbm, qgain_hbm, kgain_hbm, hgain_hbm, bias_hbm,
    out_ref, consts_ref,
    x_ref, gain_ref, wq_ref, wk_ref, wv_ref, wf_ref, qgain_ref, kgain_ref, hgain_ref, bias_ref, sems,
):
    kv = lax.axis_index("kv")
    tp = lax.axis_index("tp")
    column = pl.multiple_of(lax.div(kv, 2) * LANES, LANES)
    pairs = (
        (x_hbm, x_ref),
        (gain_hbm, gain_ref),
        (wq_hbm, wq_ref),
        (wk_hbm, wk_ref),
        (wv_hbm, wv_ref),
        (wf_hbm.at[:, pl.ds(column, LANES)], wf_ref),
        (qgain_hbm, qgain_ref),
        (kgain_hbm, kgain_ref),
        (hgain_hbm, hgain_ref),
        (bias_hbm, bias_ref),
    )
    copies = [pltpu.make_async_copy(a, b, sems.at[n]) for n, (a, b) in enumerate(pairs)]
    for copy in copies:
        copy.start()
    for copy in copies:
        copy.wait()
    at = tp * HEADS + 2 * lax.rem(kv, QUARTERS)
    spot = iota((1, 2 * HEADS), 1)
    left = iota((1, LANES), 1) < DH
    first = jnp.sum(jnp.where(spot == at, bias_ref[...], 0.0), axis=1, keepdims=True)
    second = jnp.sum(jnp.where(spot == at + 1, bias_ref[...], 0.0), axis=1, keepdims=True)
    consts_ref[0:1] = doubled(qgain_ref)
    consts_ref[1:2] = doubled(kgain_ref)
    consts_ref[2:3] = doubled(hgain_ref)
    consts_ref[3:4] = jnp.where(left, first, second)
    x = x_ref[...].reshape(ROWS, DH).astype(F32)
    scaled = (x * gain_ref[...]).astype(BF16)
    blocks = [dot_nn(scaled, w[...]) for w in (wq_ref, wk_ref, wv_ref)]
    wide = jnp.concatenate([scaled, scaled], axis=1)
    half = (iota((ROWS, LANES), 1) // DH == lax.rem(kv, 2)).astype(F32).astype(BF16)
    gates = dot_nt(wf_ref[...], wide * half)
    own = jnp.where(tp == 0, gates[:HEADS], gates[HEADS:])
    squares = jnp.sum(x * x, axis=1, keepdims=True)
    diagonal = iota((ROWS, LANES), 0) == iota((ROWS, LANES), 1)
    square_row = jnp.sum(jnp.where(diagonal, squares, 0.0), axis=0, keepdims=True)
    for c in range(QUARTERS):
        gate_row = jnp.concatenate([own[2 * c : 2 * c + 1], own[2 * c + 1 : 2 * c + 2]], axis=1)
        tail = jnp.concatenate([gate_row, square_row], axis=0)
        for g in range(GROUPS):
            at = SEND_A * (g * QUARTERS + c)
            for i, block in enumerate(blocks):
                out_ref[at + SUB * i : at + SUB * i + SUB, :] = block[
                    SUB * g : SUB * g + SUB, LANES * c : LANES * c + LANES
                ]
            out_ref[at + 24 : at + 26, :] = tail


def head_scale(block):
    left = iota(block.shape, 1) < DH
    square = block * block
    first = jnp.sum(jnp.where(left, square, 0.0), axis=1, keepdims=True)
    second = jnp.sum(jnp.where(left, 0.0, square), axis=1, keepdims=True)
    return lax.rsqrt(jnp.where(left, first, second) / DH + EPSILON)


def finish_kernel(got_ref, consts_ref, out_ref, gate_ref):
    group = lax.div(lax.axis_index("kv"), QUARTERS)
    sums = [got_ref[0:8], got_ref[8:16], got_ref[16:24], got_ref[24:26]]
    for p in range(1, N_KV):
        at = SEND_A * p
        for i in range(3):
            sums[i] = sums[i] + got_ref[at + SUB * i : at + SUB * i + SUB]
        sums[3] = sums[3] + got_ref[at + 24 : at + 26]
    gate_sum = sums[3][0:1]
    square = sums[3][1:2]
    inverse_row = lax.rsqrt(square / (N_KV * DH) + EPSILON)
    lane = iota((SUB, LANES), 1)
    pick = lane == iota((SUB, LANES), 0) + group * SUB
    inverse = jnp.sum(jnp.where(pick, inverse_row, 0.0), axis=1, keepdims=True)
    query = sums[0] * inverse
    key = sums[1] * inverse
    value = sums[2] * inverse
    query = query * head_scale(query) * consts_ref[0:1]
    key = key * head_scale(key) * consts_ref[1:2]
    twice = jnp.concatenate([inverse_row[:, :DH], inverse_row[:, :DH]], axis=1)
    logit = gate_sum * twice + consts_ref[3:4]
    small = jnp.exp(-jnp.abs(logit))
    one_more = 1.0 + small
    grown = jnp.where(
        one_more == 1.0, small, jnp.log(one_more) * small / jnp.where(one_more == 1.0, 1.0, one_more - 1.0)
    )
    gate = jnp.minimum(logit, 0.0) - grown
    gate_ref[...] = gate
    high, middle, low = pieces(gate)
    row = iota((SUB, LANES), 0)
    tail = jnp.where(row == 0, high, jnp.where(row == 1, middle, jnp.where(row == 2, low, 0.0)))
    whole = jnp.concatenate([query, key, value, tail], axis=0).astype(BF16)
    for p in range(N_KV):
        out_ref[p] = whole


def stage_kernel(key_hbm, value_hbm, gate_hbm, key_ref, value_ref, gate_ref, new_key_hbm, new_value_hbm, sems):
    loads = []
    for s in range(SEQS):
        for n, (source, target) in enumerate(((key_hbm, key_ref), (value_hbm, value_ref))):
            loads.append(pltpu.make_async_copy(source.at[s], target.at[s], sems.at[n, s]))
    gate_load = pltpu.make_async_copy(gate_hbm, gate_ref, sems.at[4, 0])
    for load in loads:
        load.start()
    gate_load.start()
    stores = []
    for s in range(SEQS):
        for n, (source, target) in enumerate(((key_ref, new_key_hbm), (value_ref, new_value_hbm))):
            loads[2 * s + n].wait()
            store = pltpu.make_async_copy(source.at[s], target.at[s], sems.at[2 + n, s])
            store.start()
            stores.append(store)
    gate_load.wait()
    for store in stores:
        store.wait()


def attend_kernel(lengths_ref, accepted_ref, got_ref, key_ref, value_ref, gate_ref, out_ref):
    for s in range(SEQS):
        attend_sequence(
            s, lengths_ref[s] + accepted_ref[s], got_ref, key_ref, value_ref, gate_ref, out_ref
        )


def attend_sequence(s, base, got_ref, key_ref, value_ref, gate_ref, out_ref):
    kv = lax.axis_index("kv")
    peer = s * 2 * QUARTERS
    query = jnp.concatenate(
        [
            jnp.concatenate([got_ref[peer + c, 0:SUB], got_ref[peer + QUARTERS + c, 0:SUB]], axis=0)
            for c in range(QUARTERS)
        ],
        axis=1,
    )
    wide = (HEADS * PROPS, WIDTH)
    own_head = iota(wide, 0) // PROPS == iota(wide, 1) // DH
    mask = jnp.where(own_head, 0.125, 0.0).astype(BF16)
    spread = jnp.concatenate([query] * HEADS, axis=0) * mask
    scores = dot_nt(spread, key_ref[s])
    gate = gate_ref[s]
    edge_hit = iota((HEADS, BLOCK), 1) + kv * BLOCK == base - 1
    edge = jnp.sum(jnp.where(edge_hit, gate, 0.0), axis=1, keepdims=True)
    gates = jnp.concatenate(
        [jnp.broadcast_to(gate[h : h + 1], (PROPS, BLOCK)) for h in range(HEADS)], axis=0
    )
    position = iota((HEADS * PROPS, BLOCK), 1) + kv * BLOCK
    live = position < base
    scores = jnp.where(live, scores - gates, MASKED)
    peak = jnp.max(scores, axis=1, keepdims=True)
    weights = jnp.where(live, jnp.exp(scores - peak), 0.0)
    total = jnp.sum(weights, axis=1, keepdims=True)
    weighted = dot_nn(weights.astype(BF16), value_ref[s])
    some = total > 0.0
    safe = jnp.where(some, total, 1.0)
    weighted = weighted * (1.0 / safe)
    log_sum = jnp.where(some, peak + jnp.log(safe), MASKED)
    lane = iota((PROPS, WIDTH), 1) // DH
    joined = jnp.zeros((PROPS, WIDTH), F32)
    for h in range(HEADS):
        joined = jnp.where(lane == h, weighted[h * PROPS : (h + 1) * PROPS], joined)
    narrow = iota((PROPS, LANES), 1)
    even = lax.rem(narrow, 2) == 0
    slot = narrow // 2
    for c in range(QUARTERS):
        first = slice(2 * c * PROPS, (2 * c + 1) * PROPS)
        second = slice((2 * c + 1) * PROPS, (2 * c + 2) * PROPS)
        sums = pieces(jnp.where(even, log_sum[first], log_sum[second]))
        edges = pieces(jnp.where(even, edge[2 * c : 2 * c + 1], edge[2 * c + 1 : 2 * c + 2]))
        extra = jnp.zeros((PROPS, LANES), F32)
        for i, piece in enumerate(sums + edges):
            extra = jnp.where(slot == i, piece, extra)
        part = joined[:, LANES * c : LANES * c + LANES]
        for e in range(2):
            out_ref[peer + e * QUARTERS + c] = jnp.concatenate(
                [part[SUB * e : SUB * e + SUB], extra[SUB * e : SUB * e + SUB]], axis=0
            ).astype(BF16)


def tree_kernel(parents_ref, gate_ref, got_ref, out_ref, gates_ref):
    kv = lax.axis_index("kv")
    group = lax.div(kv, QUARTERS)
    quarter = lax.rem(kv, QUARTERS)
    s = lax.div(group, 2)
    half = lax.rem(group, 2)
    square = (PROPS, PROPS)
    parents = parents_ref[pl.ds(s, 1), :]
    step = (iota(square, 0) == parents).astype(F32)
    identity = (iota(square, 0) == iota(square, 1)).astype(F32)
    above = identity + step
    reach = step
    for _ in range(3):
        reach = dot_nn(reach, reach)
        above = above + dot_nn(above, reach)
    lane = iota((2 * PROPS, LANES), 1)
    line = iota((2 * PROPS, LANES), 0)
    wanted = lane == (line // PROPS) * DH + s * PROPS + lax.rem(line, PROPS)
    gate = jnp.sum(jnp.where(wanted, gate_ref[...], 0.0), axis=1, keepdims=True)
    path = [
        jnp.sum(above * gate[PROPS * j : PROPS * j + PROPS], axis=0, keepdims=True) for j in range(2)
    ]
    query = got_ref[group * QUARTERS + quarter, 0:SUB].astype(F32)
    upper = s * 2 * QUARTERS + quarter
    lower = upper + QUARTERS
    keys = jnp.concatenate([got_ref[upper, 8:16], got_ref[lower, 8:16]], axis=0)
    values = jnp.concatenate([got_ref[upper, 16:24], got_ref[lower, 16:24]], axis=0)
    left = iota((SUB, LANES), 1) < DH
    spread = jnp.concatenate([jnp.where(left, query, 0.0), jnp.where(left, 0.0, query)], axis=0)
    scores = dot_nt(spread.astype(BF16), keys) * 0.125
    first = iota(square, 0) < SUB
    scores = scores - jnp.where(first, path[0], path[1])
    chosen = (iota(square, 1) == lax.rem(iota(square, 0), SUB) + half * SUB).astype(F32)
    live = dot_nt(chosen, above) > 0.5
    scores = jnp.where(live, scores, MASKED)
    peak = jnp.max(scores, axis=1, keepdims=True)
    weights = jnp.where(live, jnp.exp(scores - peak), 0.0)
    total = jnp.sum(weights, axis=1, keepdims=True)
    weighted = dot_nn(weights.astype(BF16), values) / total
    log_sum = peak + jnp.log(total)
    out_ref[0:SUB] = jnp.where(left, weighted[:SUB], weighted[SUB:])
    out_ref[SUB:] = jnp.where(left, log_sum[:SUB], log_sum[SUB:])
    for c in range(QUARTERS):
        gate = jnp.sum(got_ref[c, 24:32].astype(F32), axis=0, keepdims=True)
        for j in range(2):
            for t in range(SEQS):
                at = DH * j + PROPS * t
                gates_ref[t, 2 * c + j : 2 * c + j + 1, :] = gate[:, at : at + PROPS]


def merge_kernel(got_ref, tree_ref, consts_ref, out_ref):
    shape = (LANES, LANES)
    source = iota(shape, 0)
    place = iota(shape, 1) // DH
    mine = lax.rem(source, 2) == place
    slot = source // 2
    sums_of = jnp.where(mine & (slot < 3), 1.0, 0.0).astype(BF16)
    edges_of = jnp.where(mine & (slot >= 3) & (slot < 6), 1.0, 0.0).astype(BF16)
    extra = got_ref[:, SUB:, :].reshape(N_KV * SUB, LANES)
    log_sums = dot_nn(extra, sums_of)
    edges = dot_nn(extra, edges_of)
    edge = edges[0:SUB]
    top = log_sums[0:SUB]
    for p in range(1, N_KV):
        edge = edge + edges[SUB * p : SUB * p + SUB]
        top = jnp.maximum(top, log_sums[SUB * p : SUB * p + SUB])
    tree_sum = tree_ref[SUB:] - edge
    top = jnp.maximum(top, tree_sum)
    weight = jnp.exp(tree_sum - top)
    below = weight
    above = weight * tree_ref[0:SUB]
    for p in range(N_KV):
        weight = jnp.exp(log_sums[SUB * p : SUB * p + SUB] - top)
        below = below + weight
        above = above + weight * got_ref[p, 0:SUB].astype(F32)
    attended = above / below
    normed = (attended * head_scale(attended) * consts_ref[2:3]).astype(BF16)
    for p in range(N_KV):
        out_ref[p] = normed


def out_kernel(got_ref, w_ref, out_ref):
    result = jnp.zeros((ROWS, DH), F32)
    for c in range(QUARTERS):
        rows = jnp.concatenate(
            [got_ref[g * QUARTERS + c].astype(F32) for g in range(GROUPS)], axis=0
        ).astype(BF16)
        result = result + dot_nt(rows, w_ref[:, LANES * c : LANES * c + LANES])
    out_ref[...] = result.astype(BF16)


def write_kernel(
    lengths_ref, accepted_ref, got_ref, key_ref, value_ref, _k, _v, new_key_hbm, new_value_hbm, rows_ref, sems
):
    kv = lax.axis_index("kv")
    window = 2 * PROPS
    for s in range(SEQS):
        first = lengths_ref[s] + accepted_ref[s] - kv * BLOCK

        @pl.when((first > -PROPS) & (first < BLOCK))
        def _():
            start = jnp.minimum(lax.div(jnp.maximum(first, 0), PROPS) * PROPS, BLOCK - window)
            start = pl.multiple_of(start, PROPS)
            slot = iota((window, PROPS), 0) + start - first
            placing = (slot == iota((window, PROPS), 1)).astype(F32).astype(BF16)
            line = iota((window, WIDTH), 0) + start - first
            hit = (line >= 0) & (line < PROPS)
            copies = []
            for i, (old_ref, new_hbm) in enumerate(((key_ref, new_key_hbm), (value_ref, new_value_hbm))):
                at = SUB * (i + 1)
                rows = jnp.concatenate(
                    [
                        jnp.concatenate(
                            [
                                got_ref[2 * s * QUARTERS + c, at : at + SUB],
                                got_ref[(2 * s + 1) * QUARTERS + c, at : at + SUB],
                            ],
                            axis=0,
                        )
                        for c in range(QUARTERS)
                    ],
                    axis=1,
                )
                written = dot_nn(placing, rows)
                old = old_ref[s, pl.ds(start, window), :].astype(F32)
                rows_ref[2 * s + i] = jnp.where(hit, written, old).astype(BF16)
                copies.append(
                    pltpu.make_async_copy(
                        rows_ref.at[2 * s + i], new_hbm.at[s, pl.ds(start, window), :], sems.at[i]
                    )
                )
            for copy in copies:
                copy.start()
            for copy in copies:
                copy.wait()


def exchange(array):
    return lax.all_to_all(array, "kv", split_axis=0, concat_axis=0, tiled=True)


def shards(
    tokens,
    norm_gain,
    w_query,
    w_key,
    w_value,
    w_forget,
    forget_bias,
    query_gain,
    key_gain,
    head_gain,
    w_out,
    key_cache,
    value_cache,
    gate_cache,
    lengths,
    accepted,
    parents,
):
    def line(gain):
        return gain.reshape(1, DH)

    def limit(size):
        return pltpu.CompilerParams(vmem_limit_bytes=size * 2**20)

    cache = jax.ShapeDtypeStruct(key_cache.shape, BF16)
    sent, consts = pl.pallas_call(
        project_kernel,
        out_shape=(
            jax.ShapeDtypeStruct((N_KV * SEND_A, LANES), F32),
            jax.ShapeDtypeStruct((SUB, LANES), F32),
        ),
        in_specs=[hbm()] * 10,
        out_specs=(vmem(), vmem()),
        scratch_shapes=[
            pltpu.VMEM((SEQS, PROPS, DH), BF16),
            pltpu.VMEM((1, DH), F32),
            pltpu.VMEM((DH, WIDTH), BF16),
            pltpu.VMEM((DH, WIDTH), BF16),
            pltpu.VMEM((DH, WIDTH), BF16),
            pltpu.VMEM((2 * HEADS, LANES), BF16),
            pltpu.VMEM((1, DH), F32),
            pltpu.VMEM((1, DH), F32),
            pltpu.VMEM((1, DH), F32),
            pltpu.VMEM((1, 2 * HEADS), F32),
            pltpu.SemaphoreType.DMA((10,)),
        ],
        cost_estimate=cost(13_000_000, 700_000),
        compiler_params=limit(8),
        name="project",
    )(
        *map(
            stay,
            (
                tokens, line(norm_gain), w_query, w_key, w_value, w_forget.T,
                line(query_gain), line(key_gain), line(head_gain), forget_bias.reshape(1, 2 * HEADS),
            ),
        )
    )
    got = exchange(sent.reshape(N_KV, 1, SEND_A * LANES)).reshape(N_KV * SEND_A, LANES)
    consts, key_cache, value_cache, gate_cache = lax.optimization_barrier(
        (consts, key_cache, value_cache, gate_cache)
    )
    keys, values, gate_block, new_keys, new_values = pl.pallas_call(
        stage_kernel,
        out_shape=(
            pltpu.VMEM(key_cache.shape, BF16),
            pltpu.VMEM(value_cache.shape, BF16),
            jax.ShapeDtypeStruct(gate_cache.shape, F32),
            pltpu.HBM(key_cache.shape, BF16),
            pltpu.HBM(value_cache.shape, BF16),
        ),
        in_specs=[hbm()] * 3,
        out_specs=(vmem(), vmem(), vmem(), hbm(), hbm()),
        scratch_shapes=[pltpu.SemaphoreType.DMA((5, SEQS))],
        cost_estimate=cost(500_000_000, 8_500_000),
        compiler_params=limit(8),
        name="stage",
    )(stay(key_cache), stay(value_cache), stay(gate_cache))
    got, keys, values = lax.optimization_barrier((got, keys, values))
    sent, gate_row = pl.pallas_call(
        finish_kernel,
        out_shape=(
            jax.ShapeDtypeStruct((N_KV, SEND_B, LANES), BF16),
            jax.ShapeDtypeStruct((1, LANES), F32),
        ),
        in_specs=[vmem(), vmem()],
        out_specs=(vmem(), vmem()),
        cost_estimate=cost(1_000_000, 700_000),
        compiler_params=limit(8),
        name="finish",
    )(got, consts)
    rows = exchange(sent)
    sent = pl.pallas_call(
        attend_kernel,
        out_shape=jax.ShapeDtypeStruct((N_KV, SEND_C, LANES), BF16),
        in_specs=[smem(), smem()] + [vmem()] * 4,
        out_specs=vmem(),
        cost_estimate=cost(600_000_000, 4_500_000),
        compiler_params=limit(16),
        name="attend",
    )(lengths, accepted, rows, close(keys), close(values), gate_block)
    got = exchange(sent)
    tree, gates = pl.pallas_call(
        tree_kernel,
        out_shape=(
            jax.ShapeDtypeStruct((2 * SUB, LANES), F32),
            jax.ShapeDtypeStruct((SEQS, HEADS, PROPS), F32),
        ),
        in_specs=[vmem()] * 3,
        out_specs=(vmem(), vmem()),
        cost_estimate=cost(2_000_000, 300_000),
        compiler_params=limit(8),
        name="tree",
    )(parents, gate_row, rows)
    new_keys, new_values = pl.pallas_call(
        write_kernel,
        out_shape=(cache, cache),
        in_specs=[smem(), smem(), vmem(), vmem(), vmem(), hbm(), hbm()],
        out_specs=(hbm(), hbm()),
        scratch_shapes=[
            pltpu.VMEM((2 * SEQS, 2 * PROPS, WIDTH), BF16),
            pltpu.SemaphoreType.DMA((2,)),
        ],
        input_output_aliases={5: 0, 6: 1},
        cost_estimate=cost(60_000_000, 8_500_000),
        compiler_params=limit(8),
        name="write",
    )(lengths, accepted, rows, close(keys), close(values), stay(new_keys), stay(new_values))
    tree, new_keys, new_values = lax.optimization_barrier((tree, new_keys, new_values))
    sent = pl.pallas_call(
        merge_kernel,
        out_shape=jax.ShapeDtypeStruct((N_KV, SUB, LANES), BF16),
        in_specs=[vmem()] * 3,
        out_specs=vmem(),
        cost_estimate=cost(8_000_000, 200_000),
        compiler_params=limit(8),
        name="merge",
    )(got, tree, consts)
    got = exchange(sent)
    term = pl.pallas_call(
        out_kernel,
        out_shape=jax.ShapeDtypeStruct((ROWS, DH), BF16),
        in_specs=[vmem()] * 2,
        out_specs=vmem(),
        cost_estimate=cost(4_000_000, 150_000),
        compiler_params=limit(8),
        name="out",
    )(got, w_out.T)
    other = lax.ppermute(term, "tp", [(0, 1), (1, 0)])
    layer_out = (term.astype(F32) + other.astype(F32)).astype(BF16)
    return (layer_out.reshape(SEQS, PROPS, DH), new_keys, new_values, gates.transpose(0, 2, 1))


def solution(mesh):
    placed = (
        P("dp", None, "kv"),
        P("kv"),
        P("kv", "tp"),
        P("kv", "tp"),
        P("kv", "tp"),
        P(),
        P(),
        P(),
        P(),
        P(),
        P("tp", "kv"),
        P("dp", "kv", "tp"),
        P("dp", "kv", "tp"),
        P("dp", "tp", "kv"),
        P("dp"),
        P("dp"),
        P("dp", None),
    )
    return jax.shard_map(
        shards,
        mesh=mesh,
        in_specs=placed,
        out_specs=(
            P("dp", None, "kv"),
            P("dp", "kv", "tp"),
            P("dp", "kv", "tp"),
            P("dp", None, "tp"),
        ),
        check_vma=False,
    )
```

```python
import jax
import jax.numpy as jnp
from jax import lax
from jax.experimental import pallas as pl
from jax.experimental.pallas import tpu as pltpu
from jax.sharding import PartitionSpec as P

EPSILON = 1e-06
MASKED = -1e30
F32 = jnp.float32
BF16 = jnp.bfloat16

LANES = 128
SUB = 8
N_KV = 32
GROUPS = 8
QUARTERS = 4
ROWS = 64
HEADS = 8
DH = 64
WIDTH = 512
PROPS = 16
SEQS = 4
BLOCK = 512
SEND_A = 26
SEND_B = 24
SEND_C = 24
HELD = 2


def iota(shape, dim):
    return lax.broadcasted_iota(jnp.int32, shape, dim)


def dot_nn(a, b):
    return lax.dot_general(a, b, (((1,), (0,)), ((), ())), preferred_element_type=F32)


def dot_nt(a, b):
    return lax.dot_general(a, b, (((1,), (1,)), ((), ())), preferred_element_type=F32)


def pieces(x):
    high = x.astype(BF16).astype(F32)
    rest = x - high
    middle = rest.astype(BF16).astype(F32)
    return high, middle, rest - middle


def vmem():
    return pl.BlockSpec(memory_space=pltpu.VMEM)


def stay(array):
    return pltpu.with_memory_space_constraint(array, pltpu.HBM)


def hbm():
    return pl.BlockSpec(memory_space=pltpu.HBM)


def smem():
    return pl.BlockSpec(memory_space=pltpu.SMEM)


def cost(flops, moved):
    return pl.CostEstimate(flops=flops, bytes_accessed=moved, transcendentals=0)


def doubled(gain_ref):
    gain = gain_ref[...]
    return jnp.concatenate([gain, gain], axis=1)


def project_kernel(
    x_hbm, gain_hbm, wq_hbm, wk_hbm, wv_hbm, wf_hbm, qgain_hbm, kgain_hbm, hgain_hbm, bias_hbm, lengths_hbm, accepted_hbm,
    out_ref, consts_ref,
    x_ref, gain_ref, wq_ref, wk_ref, wv_ref, wf_ref, qgain_ref, kgain_ref, hgain_ref, bias_ref, lengths_ref, accepted_ref, sems,
):
    kv = lax.axis_index("kv")
    tp = lax.axis_index("tp")
    column = pl.multiple_of(lax.div(kv, 2) * LANES, LANES)
    pairs = (
        (x_hbm, x_ref),
        (gain_hbm, gain_ref),
        (wq_hbm, wq_ref),
        (wk_hbm, wk_ref),
        (wv_hbm, wv_ref),
        (wf_hbm.at[:, pl.ds(column, LANES)], wf_ref),
        (qgain_hbm, qgain_ref),
        (kgain_hbm, kgain_ref),
        (hgain_hbm, hgain_ref),
        (bias_hbm, bias_ref),
        (lengths_hbm, lengths_ref),
        (accepted_hbm, accepted_ref),
    )
    copies = [pltpu.make_async_copy(a, b, sems.at[n]) for n, (a, b) in enumerate(pairs)]
    for copy in copies:
        copy.start()
    for copy in copies:
        copy.wait()
    at = tp * HEADS + 2 * lax.rem(kv, QUARTERS)
    spot = iota((1, 2 * HEADS), 1)
    left = iota((1, LANES), 1) < DH
    first = jnp.sum(jnp.where(spot == at, bias_ref[...], 0.0), axis=1, keepdims=True)
    second = jnp.sum(jnp.where(spot == at + 1, bias_ref[...], 0.0), axis=1, keepdims=True)
    consts_ref[0:1] = doubled(qgain_ref)
    consts_ref[1:2] = doubled(kgain_ref)
    consts_ref[2:3] = doubled(hgain_ref)
    consts_ref[3:4] = jnp.where(left, first, second)
    consts_ref[4:5, 0:SEQS] = (lengths_ref[...] + accepted_ref[...]).astype(F32)
    x = x_ref[...].reshape(ROWS, DH).astype(F32)
    scaled = (x * gain_ref[...]).astype(BF16)
    blocks = [dot_nn(scaled, w[...]) for w in (wq_ref, wk_ref, wv_ref)]
    wide = jnp.concatenate([scaled, scaled], axis=1)
    half = (iota((ROWS, LANES), 1) // DH == lax.rem(kv, 2)).astype(F32).astype(BF16)
    gates = dot_nt(wf_ref[...], wide * half)
    own = jnp.where(tp == 0, gates[:HEADS], gates[HEADS:])
    squares = jnp.sum(x * x, axis=1, keepdims=True)
    diagonal = iota((ROWS, LANES), 0) == iota((ROWS, LANES), 1)
    square_row = jnp.sum(jnp.where(diagonal, squares, 0.0), axis=0, keepdims=True)
    for c in range(QUARTERS):
        gate_row = jnp.concatenate([own[2 * c : 2 * c + 1], own[2 * c + 1 : 2 * c + 2]], axis=1)
        tail = jnp.concatenate([gate_row, square_row], axis=0)
        for g in range(GROUPS):
            at = SEND_A * (g * QUARTERS + c)
            for i, block in enumerate(blocks):
                out_ref[at + SUB * i : at + SUB * i + SUB, :] = block[
                    SUB * g : SUB * g + SUB, LANES * c : LANES * c + LANES
                ]
            out_ref[at + 24 : at + 26, :] = tail


def head_scale(block):
    left = iota(block.shape, 1) < DH
    square = block * block
    first = jnp.sum(jnp.where(left, square, 0.0), axis=1, keepdims=True)
    second = jnp.sum(jnp.where(left, 0.0, square), axis=1, keepdims=True)
    return lax.rsqrt(jnp.where(left, first, second) / DH + EPSILON)


def finish_kernel(got_ref, consts_ref, out_ref, gate_ref):
    group = lax.div(lax.axis_index("kv"), QUARTERS)
    sums = [got_ref[0:8], got_ref[8:16], got_ref[16:24], got_ref[24:26]]
    for p in range(1, N_KV):
        at = SEND_A * p
        for i in range(3):
            sums[i] = sums[i] + got_ref[at + SUB * i : at + SUB * i + SUB]
        sums[3] = sums[3] + got_ref[at + 24 : at + 26]
    gate_sum = sums[3][0:1]
    square = sums[3][1:2]
    inverse_row = lax.rsqrt(square / (N_KV * DH) + EPSILON)
    lane = iota((SUB, LANES), 1)
    pick = lane == iota((SUB, LANES), 0) + group * SUB
    inverse = jnp.sum(jnp.where(pick, inverse_row, 0.0), axis=1, keepdims=True)
    query = sums[0] * inverse
    key = sums[1] * inverse
    value = sums[2] * inverse
    query = query * head_scale(query) * consts_ref[0:1]
    key = key * head_scale(key) * consts_ref[1:2]
    twice = jnp.concatenate([inverse_row[:, :DH], inverse_row[:, :DH]], axis=1)
    logit = gate_sum * twice + consts_ref[3:4]
    small = jnp.exp(-jnp.abs(logit))
    one_more = 1.0 + small
    grown = jnp.where(
        one_more == 1.0, small, jnp.log(one_more) * small / jnp.where(one_more == 1.0, 1.0, one_more - 1.0)
    )
    gate = jnp.minimum(logit, 0.0) - grown
    gate_ref[...] = gate
    whole = jnp.concatenate([query, key, value], axis=0).astype(BF16)
    for p in range(N_KV):
        out_ref[p] = whole


def stage_kernel(
    key_hbm, value_hbm, gate_hbm, key_ref, held_ref, gate_ref, new_key_hbm, new_value_hbm, rest_ref, sems
):
    gate_load = pltpu.make_async_copy(gate_hbm, gate_ref, sems.at[2, 0])
    gate_load.start()
    targets = [key_ref.at[s] for s in range(SEQS)]
    targets += [held_ref.at[s] if s < HELD else rest_ref.at[s - HELD] for s in range(SEQS)]
    sources = [key_hbm.at[s] for s in range(SEQS)] + [value_hbm.at[s] for s in range(SEQS)]
    news = [new_key_hbm.at[s] for s in range(SEQS)] + [new_value_hbm.at[s] for s in range(SEQS)]
    loads = [pltpu.make_async_copy(a, b, sems.at[0, n]) for n, (a, b) in enumerate(zip(sources, targets))]
    stores = [pltpu.make_async_copy(a, b, sems.at[1, n]) for n, (a, b) in enumerate(zip(targets, news))]
    for load in loads:
        load.start()
    for load, store in zip(loads, stores):
        load.wait()
        store.start()
    gate_load.wait()
    for store in stores:
        store.wait()


def attend_kernel(
    consts_ref, row_ref, parents_ref, got_ref, key_ref, held_ref, gate_ref, value_hbm,
    out_ref, tree_ref, rest_ref, weights_ref, sems,
):
    loads = {}
    for s in range(HELD, SEQS):
        loads[s] = pltpu.make_async_copy(value_hbm.at[s], rest_ref.at[s - HELD], sems.at[s])
        loads[s].start()
    tail = gate_tail(row_ref)
    attend_tree(parents_ref, row_ref, got_ref, tree_ref)
    sums = []
    for s in range(SEQS):
        raw = score_sequence(s, got_ref, key_ref)
        sums.append(weigh_sequence(s, raw, consts_ref[4:5, s : s + 1], gate_ref, weights_ref))
    for s in range(SEQS):
        if s in loads:
            loads[s].wait()
        values = held_ref[s] if s < HELD else rest_ref[s - HELD]
        send_sequence(s, dot_nn(weights_ref[s], values), *sums[s], tail, out_ref)


def gate_tail(row_ref):
    shape = (LANES, LANES)
    narrow = lax.rem(iota(shape, 0), PROPS) == lax.rem(iota(shape, 1), PROPS)
    slot = iota(shape, 1) // PROPS
    mine = iota((SUB, LANES), 1) // PROPS == iota((SUB, LANES), 0)
    tail = jnp.zeros((SUB, LANES), F32)
    for i, piece in enumerate(pieces(row_ref[...])):
        move = jnp.where(narrow & (slot == i + 1), 1.0, 0.0).astype(BF16)
        tail = tail + dot_nn(jnp.where(mine, piece, 0.0).astype(BF16), move)
    return tail


def score_sequence(s, got_ref, key_ref):
    peer = s * 2 * QUARTERS
    query = jnp.concatenate(
        [
            jnp.concatenate([got_ref[peer + c, 0:SUB], got_ref[peer + QUARTERS + c, 0:SUB]], axis=0)
            for c in range(QUARTERS)
        ],
        axis=1,
    )
    wide = (HEADS * PROPS, WIDTH)
    own_head = iota(wide, 0) // PROPS == iota(wide, 1) // DH
    mask = jnp.where(own_head, 0.125, 0.0).astype(BF16)
    spread = jnp.concatenate([query] * HEADS, axis=0) * mask
    return dot_nt(spread, key_ref[s])


def weigh_sequence(s, scores, base, gate_ref, weights_ref):
    kv = lax.axis_index("kv")
    gate = gate_ref[s]
    edge_hit = (iota((HEADS, BLOCK), 1) + (kv * BLOCK + 1)).astype(F32) == base
    edge = jnp.sum(jnp.where(edge_hit, gate, 0.0), axis=1, keepdims=True)
    gates = jnp.concatenate(
        [jnp.broadcast_to(gate[h : h + 1], (PROPS, BLOCK)) for h in range(HEADS)], axis=0
    )
    position = (iota((HEADS * PROPS, BLOCK), 1) + kv * BLOCK).astype(F32)
    live = position < base
    scores = jnp.where(live, scores - gates, MASKED)
    peak = jnp.max(scores, axis=1, keepdims=True)
    weights = jnp.where(live, jnp.exp(scores - peak), 0.0)
    total = jnp.sum(weights, axis=1, keepdims=True)
    weights_ref[s] = weights.astype(BF16)
    some = total > 0.0
    safe = jnp.where(some, total, 1.0)
    log_sum = jnp.where(some, peak + jnp.log(safe), MASKED)
    return 1.0 / safe, log_sum, edge


def send_sequence(s, weighted, scale, log_sum, edge, tail, out_ref):
    peer = s * 2 * QUARTERS
    weighted = weighted * scale
    lane = iota((PROPS, WIDTH), 1) // DH
    joined = jnp.zeros((PROPS, WIDTH), F32)
    for h in range(HEADS):
        joined = jnp.where(lane == h, weighted[h * PROPS : (h + 1) * PROPS], joined)
    narrow = iota((PROPS, LANES), 1)
    even = lax.rem(narrow, 2) == 0
    slot = narrow // 2
    for c in range(QUARTERS):
        first = slice(2 * c * PROPS, (2 * c + 1) * PROPS)
        second = slice((2 * c + 1) * PROPS, (2 * c + 2) * PROPS)
        sums = pieces(jnp.where(even, log_sum[first], log_sum[second]))
        edges = pieces(jnp.where(even, edge[2 * c : 2 * c + 1], edge[2 * c + 1 : 2 * c + 2]))
        extra = jnp.concatenate([tail, tail], axis=0)
        for i, piece in enumerate(sums + edges):
            extra = jnp.where(slot == i, piece, extra)
        part = joined[:, LANES * c : LANES * c + LANES]
        high = part.astype(BF16).astype(F32)
        low = part - high
        for e in range(2):
            rows = slice(SUB * e, SUB * e + SUB)
            out_ref[peer + e * QUARTERS + c] = jnp.concatenate(
                [high[rows], low[rows], extra[rows]], axis=0
            ).astype(BF16)


def attend_tree(parents_ref, gate_ref, got_ref, out_ref):
    kv = lax.axis_index("kv")
    group = lax.div(kv, QUARTERS)
    quarter = lax.rem(kv, QUARTERS)
    s = lax.div(group, 2)
    half = lax.rem(group, 2)
    square = (PROPS, PROPS)
    parents = parents_ref[pl.ds(s, 1), :]
    step = (iota(square, 0) == parents).astype(F32)
    identity = (iota(square, 0) == iota(square, 1)).astype(F32)
    above = identity + step
    reach = step
    for _ in range(3):
        reach = dot_nn(reach, reach)
        above = above + dot_nn(above, reach)
    lane = iota((2 * PROPS, LANES), 1)
    line = iota((2 * PROPS, LANES), 0)
    wanted = lane == (line // PROPS) * DH + s * PROPS + lax.rem(line, PROPS)
    gate = jnp.sum(jnp.where(wanted, gate_ref[...], 0.0), axis=1, keepdims=True)
    path = [
        jnp.sum(above * gate[PROPS * j : PROPS * j + PROPS], axis=0, keepdims=True) for j in range(2)
    ]
    query = got_ref[group * QUARTERS + quarter, 0:SUB].astype(F32)
    upper = s * 2 * QUARTERS + quarter
    lower = upper + QUARTERS
    keys = jnp.concatenate([got_ref[upper, 8:16], got_ref[lower, 8:16]], axis=0)
    values = jnp.concatenate([got_ref[upper, 16:24], got_ref[lower, 16:24]], axis=0)
    left = iota((SUB, LANES), 1) < DH
    spread = jnp.concatenate([jnp.where(left, query, 0.0), jnp.where(left, 0.0, query)], axis=0)
    scores = dot_nt(spread.astype(BF16), keys) * 0.125
    first = iota(square, 0) < SUB
    scores = scores - jnp.where(first, path[0], path[1])
    chosen = (iota(square, 1) == lax.rem(iota(square, 0), SUB) + half * SUB).astype(F32)
    live = dot_nt(chosen, above) > 0.5
    scores = jnp.where(live, scores, MASKED)
    peak = jnp.max(scores, axis=1, keepdims=True)
    weights = jnp.where(live, jnp.exp(scores - peak), 0.0)
    total = jnp.sum(weights, axis=1, keepdims=True)
    weighted = dot_nn(weights.astype(BF16), values) / total
    log_sum = peak + jnp.log(total)
    out_ref[0:SUB] = jnp.where(left, weighted[:SUB], weighted[SUB:])
    out_ref[SUB:] = jnp.where(left, log_sum[:SUB], log_sum[SUB:])


def merge_kernel(got_ref, tree_ref, consts_ref, out_ref):
    shape = (LANES, LANES)
    source = iota(shape, 0)
    place = iota(shape, 1) // DH
    mine = lax.rem(source, 2) == place
    slot = source // 2
    sums_of = jnp.where(mine & (slot < 3), 1.0, 0.0).astype(BF16)
    edges_of = jnp.where(mine & (slot >= 3) & (slot < 6), 1.0, 0.0).astype(BF16)
    extra = got_ref[:, 2 * SUB :, :].reshape(N_KV * SUB, LANES)
    log_sums = dot_nn(extra, sums_of)
    edges = dot_nn(extra, edges_of)
    edge = edges[0:SUB]
    top = log_sums[0:SUB]
    for p in range(1, N_KV):
        edge = edge + edges[SUB * p : SUB * p + SUB]
        top = jnp.maximum(top, log_sums[SUB * p : SUB * p + SUB])
    tree_sum = tree_ref[SUB:] - edge
    top = jnp.maximum(top, tree_sum)
    weight = jnp.exp(tree_sum - top)
    below = weight
    above = weight * tree_ref[0:SUB]
    for p in range(N_KV):
        weight = jnp.exp(log_sums[SUB * p : SUB * p + SUB] - top)
        below = below + weight
        part = got_ref[p, 0:SUB].astype(F32) + got_ref[p, SUB : 2 * SUB].astype(F32)
        above = above + weight * part
    attended = above / below
    normed = attended * head_scale(attended) * consts_ref[2:3]
    whole = normed.astype(BF16)
    for p in range(N_KV):
        out_ref[p] = whole


def out_kernel(got_ref, w_ref, out_ref):
    result = jnp.zeros((ROWS, DH), F32)
    for c in range(QUARTERS):
        rows = jnp.concatenate(
            [got_ref[g * QUARTERS + c].astype(F32) for g in range(GROUPS)], axis=0
        ).astype(BF16)
        result = result + dot_nt(rows, w_ref[:, LANES * c : LANES * c + LANES])
    out_ref[...] = result.astype(BF16)


def write_kernel(
    lengths_ref, accepted_ref, parts_ref, got_ref, key_hbm, value_hbm, _k, _v,
    new_key_hbm, new_value_hbm, gates_ref, old_ref, rows_ref, sems,
):
    kv = lax.axis_index("kv")
    window = 2 * PROPS
    firsts = [lengths_ref[s] + accepted_ref[s] - kv * BLOCK for s in range(SEQS)]
    mine = [(first > -PROPS) & (first < BLOCK) for first in firsts]
    starts = [
        pl.multiple_of(jnp.minimum(lax.div(jnp.maximum(first, 0), PROPS) * PROPS, BLOCK - window), PROPS)
        for first in firsts
    ]

    def load(s, i):
        source = (key_hbm, value_hbm)[i].at[s, pl.ds(starts[s], window), :]
        return pltpu.make_async_copy(source, old_ref.at[2 * s + i], sems.at[0, 2 * s + i])

    def store(s, i):
        target = (new_key_hbm, new_value_hbm)[i].at[s, pl.ds(starts[s], window), :]
        return pltpu.make_async_copy(rows_ref.at[2 * s + i], target, sems.at[1, 2 * s + i])

    for s in range(SEQS):

        @pl.when(mine[s])
        def _():
            for i in range(2):
                load(s, i).start()

    for c in range(QUARTERS):
        extra = parts_ref[c, 2 * SUB : 3 * SUB].astype(F32)
        gate = extra[:, PROPS : 2 * PROPS]
        for i in (2, 3):
            gate = gate + extra[:, PROPS * i : PROPS * (i + 1)]
        for j in range(2):
            for t in range(SEQS):
                at = SEQS * j + t
                gates_ref[t, 2 * c + j : 2 * c + j + 1, :] = gate[at : at + 1]
    for s in range(SEQS):

        @pl.when(mine[s])
        def _():
            offset = starts[s] - firsts[s]
            placing = (iota((window, PROPS), 0) + offset == iota((window, PROPS), 1)).astype(F32).astype(BF16)
            line = iota((window, WIDTH), 0) + offset
            hit = (line >= 0) & (line < PROPS)
            for i in range(2):
                at = SUB * (i + 1)
                rows = jnp.concatenate(
                    [
                        jnp.concatenate(
                            [
                                got_ref[2 * s * QUARTERS + c, at : at + SUB],
                                got_ref[(2 * s + 1) * QUARTERS + c, at : at + SUB],
                            ],
                            axis=0,
                        )
                        for c in range(QUARTERS)
                    ],
                    axis=1,
                )
                written = dot_nn(placing, rows)
                load(s, i).wait()
                old = old_ref[2 * s + i].astype(F32)
                rows_ref[2 * s + i] = jnp.where(hit, written, old).astype(BF16)
                store(s, i).start()

    for s in range(SEQS):

        @pl.when(mine[s])
        def _():
            for i in range(2):
                store(s, i).wait()


def exchange(array):
    return lax.all_to_all(array, "kv", split_axis=0, concat_axis=0, tiled=True)


def shards(
    tokens,
    norm_gain,
    w_query,
    w_key,
    w_value,
    w_forget,
    forget_bias,
    query_gain,
    key_gain,
    head_gain,
    w_out,
    key_cache,
    value_cache,
    gate_cache,
    lengths,
    accepted,
    parents,
):
    def line(gain):
        return gain.reshape(1, DH)

    def limit(size):
        return pltpu.CompilerParams(vmem_limit_bytes=size * 2**20)

    cache = jax.ShapeDtypeStruct(key_cache.shape, BF16)
    sent, consts = pl.pallas_call(
        project_kernel,
        out_shape=(
            jax.ShapeDtypeStruct((N_KV * SEND_A, LANES), F32),
            jax.ShapeDtypeStruct((SUB, LANES), F32),
        ),
        in_specs=[hbm()] * 12,
        out_specs=(vmem(), vmem()),
        scratch_shapes=[
            pltpu.VMEM((SEQS, PROPS, DH), BF16),
            pltpu.VMEM((1, DH), F32),
            pltpu.VMEM((DH, WIDTH), BF16),
            pltpu.VMEM((DH, WIDTH), BF16),
            pltpu.VMEM((DH, WIDTH), BF16),
            pltpu.VMEM((2 * HEADS, LANES), BF16),
            pltpu.VMEM((1, DH), F32),
            pltpu.VMEM((1, DH), F32),
            pltpu.VMEM((1, DH), F32),
            pltpu.VMEM((1, 2 * HEADS), F32),
            pltpu.VMEM((1, SEQS), jnp.int32),
            pltpu.VMEM((1, SEQS), jnp.int32),
            pltpu.SemaphoreType.DMA((12,)),
        ],
        cost_estimate=cost(13_000_000, 700_000),
        compiler_params=limit(8),
        name="project",
    )(
        *map(
            stay,
            (
                tokens, line(norm_gain), w_query, w_key, w_value, w_forget.T,
                line(query_gain), line(key_gain), line(head_gain), forget_bias.reshape(1, 2 * HEADS),
                lengths.reshape(1, SEQS), accepted.reshape(1, SEQS),
            ),
        )
    )
    got = exchange(sent.reshape(N_KV, 1, SEND_A * LANES)).reshape(N_KV * SEND_A, LANES)
    sent, gate_row = pl.pallas_call(
        finish_kernel,
        out_shape=(
            jax.ShapeDtypeStruct((N_KV, SEND_B, LANES), BF16),
            jax.ShapeDtypeStruct((1, LANES), F32),
        ),
        in_specs=[vmem(), vmem()],
        out_specs=(vmem(), vmem()),
        cost_estimate=cost(1_000_000, 700_000),
        compiler_params=limit(8),
        name="finish",
    )(got, consts)
    rows = exchange(sent)
    gate_row, key_cache, value_cache, gate_cache = lax.optimization_barrier(
        (gate_row, key_cache, value_cache, gate_cache)
    )
    keys, held, gate_block, new_keys, new_values = pl.pallas_call(
        stage_kernel,
        out_shape=(
            cache,
            jax.ShapeDtypeStruct((HELD, BLOCK, WIDTH), BF16),
            jax.ShapeDtypeStruct(gate_cache.shape, F32),
            pltpu.HBM(key_cache.shape, BF16),
            pltpu.HBM(value_cache.shape, BF16),
        ),
        in_specs=[hbm()] * 3,
        out_specs=(vmem(), vmem(), vmem(), hbm(), hbm()),
        scratch_shapes=[
            pltpu.VMEM((SEQS - HELD, BLOCK, WIDTH), BF16),
            pltpu.SemaphoreType.DMA((3, 2 * SEQS)),
        ],
        cost_estimate=cost(500_000_000, 8_500_000),
        compiler_params=limit(8),
        name="stage",
    )(stay(key_cache), stay(value_cache), stay(gate_cache))
    rows, keys, held, gate_block = lax.optimization_barrier((rows, keys, held, gate_block))
    sent, tree = pl.pallas_call(
        attend_kernel,
        out_shape=(
            jax.ShapeDtypeStruct((N_KV, SEND_C, LANES), BF16),
            jax.ShapeDtypeStruct((2 * SUB, LANES), F32),
        ),
        in_specs=[vmem()] * 7 + [hbm()],
        out_specs=(vmem(), vmem()),
        scratch_shapes=[
            pltpu.VMEM((SEQS - HELD, BLOCK, WIDTH), BF16),
            pltpu.VMEM((SEQS, HEADS * PROPS, BLOCK), BF16),
            pltpu.SemaphoreType.DMA((SEQS + 1,)),
        ],
        cost_estimate=cost(600_000_000, 4_500_000),
        compiler_params=limit(16),
        name="attend",
    )(consts, gate_row, parents, rows, keys, held, gate_block, stay(value_cache))
    parts = exchange(sent)
    sent = pl.pallas_call(
        merge_kernel,
        out_shape=jax.ShapeDtypeStruct((N_KV, SUB, LANES), BF16),
        in_specs=[vmem()] * 3,
        out_specs=vmem(),
        cost_estimate=cost(8_000_000, 200_000),
        compiler_params=limit(8),
        name="merge",
    )(parts, tree, consts)
    normed = exchange(sent)
    term = pl.pallas_call(
        out_kernel,
        out_shape=jax.ShapeDtypeStruct((ROWS, DH), BF16),
        in_specs=[vmem()] * 2,
        out_specs=vmem(),
        cost_estimate=cost(4_000_000, 150_000),
        compiler_params=limit(8),
        name="out",
    )(normed, w_out.T)
    other = lax.ppermute(term, "tp", [(0, 1), (1, 0)])
    term, parts = lax.optimization_barrier((term, parts))
    new_keys, new_values, gates = pl.pallas_call(
        write_kernel,
        out_shape=(cache, cache, jax.ShapeDtypeStruct((SEQS, HEADS, PROPS), F32)),
        in_specs=[smem(), smem(), vmem(), vmem()] + [hbm()] * 4,
        out_specs=(hbm(), hbm(), vmem()),
        scratch_shapes=[
            pltpu.VMEM((2 * SEQS, 2 * PROPS, WIDTH), BF16),
            pltpu.VMEM((2 * SEQS, 2 * PROPS, WIDTH), BF16),
            pltpu.SemaphoreType.DMA((2, 2 * SEQS)),
        ],
        input_output_aliases={6: 0, 7: 1},
        cost_estimate=cost(60_000_000, 1_000_000),
        compiler_params=limit(8),
        name="write",
    )(
        lengths, accepted, parts, rows, stay(key_cache), stay(value_cache), stay(new_keys), stay(new_values)
    )
    layer_out = (term.astype(F32) + other.astype(F32)).astype(BF16)
    return (layer_out.reshape(SEQS, PROPS, DH), new_keys, new_values, gates.transpose(0, 2, 1))


def solution(mesh):
    placed = (
        P("dp", None, "kv"),
        P("kv"),
        P("kv", "tp"),
        P("kv", "tp"),
        P("kv", "tp"),
        P(),
        P(),
        P(),
        P(),
        P(),
        P("tp", "kv"),
        P("dp", "kv", "tp"),
        P("dp", "kv", "tp"),
        P("dp", "tp", "kv"),
        P("dp"),
        P("dp"),
        P("dp", None),
    )
    return jax.shard_map(
        shards,
        mesh=mesh,
        in_specs=placed,
        out_specs=(
            P("dp", None, "kv"),
            P("dp", "kv", "tp"),
            P("dp", "kv", "tp"),
            P("dp", None, "tp"),
        ),
        check_vma=False,
    )
```

```python
import jax
import jax.numpy as jnp
from jax import lax
from jax.experimental import pallas as pl
from jax.experimental.pallas import tpu as pltpu
from jax.sharding import PartitionSpec as P

EPSILON = 1e-06
MASKED = -1e30
F32 = jnp.float32
BF16 = jnp.bfloat16

LANES = 128
SUB = 8
N_KV = 32
QUARTERS = 4
ROWS = 64
HEADS = 8
DH = 64
WIDTH = 512
PROPS = 16
SEQS = 4
BLOCK = 512
SEND_A = 9
SEND_KV = 24
SEND_B = SUB + SEND_KV
SEND_C = 9
SEND_D = 24
HELD = 2


def iota(shape, dim):
    return lax.broadcasted_iota(jnp.int32, shape, dim)


def dot_nn(a, b):
    return lax.dot_general(a, b, (((1,), (0,)), ((), ())), preferred_element_type=F32)


def dot_nt(a, b):
    return lax.dot_general(a, b, (((1,), (1,)), ((), ())), preferred_element_type=F32)


def pieces(x):
    high = x.astype(BF16).astype(F32)
    rest = x - high
    middle = rest.astype(BF16).astype(F32)
    return high, middle, rest - middle


def left_of(shape):
    return iota(shape, len(shape) - 1) < DH


def swapped(block):
    return pltpu.roll(block, DH, 1)


def packed(top, bottom):
    left = left_of(top.shape)
    return jnp.where(left, top, swapped(bottom)), jnp.where(left, swapped(top), bottom)


def unpacked_rows(read, s):
    tiles = []
    for c in range(QUARTERS):
        even, odd = (read(s * HEADS + 2 * c + j).astype(F32) for j in range(2))
        tiles.append(jnp.concatenate(packed(even, odd), axis=0))
    return jnp.concatenate(tiles, axis=1).astype(BF16)


def vmem():
    return pl.BlockSpec(memory_space=pltpu.VMEM)


def stay(array):
    return pltpu.with_memory_space_constraint(array, pltpu.HBM)


def hbm():
    return pl.BlockSpec(memory_space=pltpu.HBM)


def cost(flops, moved):
    return pl.CostEstimate(flops=flops, bytes_accessed=moved, transcendentals=0)


def doubled(gain_ref):
    gain = gain_ref[...]
    return jnp.concatenate([gain, gain], axis=1)


def project_kernel(
    x_hbm, gain_hbm, wq_hbm, wk_hbm, wv_hbm, wf_hbm, qgain_hbm, kgain_hbm, hgain_hbm, bias_hbm, lengths_hbm, accepted_hbm,
    out_ref, part_ref, consts_ref,
    x_ref, gain_ref, wq_ref, wk_ref, wv_ref, wf_ref, qgain_ref, kgain_ref, hgain_ref, bias_ref, lengths_ref, accepted_ref, sems,
):
    kv = lax.axis_index("kv")
    tp = lax.axis_index("tp")
    column = pl.multiple_of(lax.div(kv, 2) * LANES, LANES)
    pairs = (
        (x_hbm, x_ref),
        (gain_hbm, gain_ref),
        (wq_hbm, wq_ref),
        (wk_hbm, wk_ref),
        (wv_hbm, wv_ref),
        (wf_hbm.at[:, pl.ds(column, LANES)], wf_ref),
        (qgain_hbm, qgain_ref),
        (kgain_hbm, kgain_ref),
        (hgain_hbm, hgain_ref),
        (bias_hbm, bias_ref),
        (lengths_hbm, lengths_ref),
        (accepted_hbm, accepted_ref),
    )
    copies = [pltpu.make_async_copy(a, b, sems.at[n]) for n, (a, b) in enumerate(pairs)]
    for copy in copies:
        copy.start()
    for copy in copies:
        copy.wait()
    at = tp * HEADS + lax.rem(kv, HEADS)
    spot = iota((1, 2 * HEADS), 1)
    bias = jnp.sum(jnp.where(spot == at, bias_ref[...], 0.0), axis=1, keepdims=True)
    consts_ref[0:1] = doubled(qgain_ref)
    consts_ref[1:2] = doubled(kgain_ref)
    consts_ref[2:3] = doubled(hgain_ref)
    consts_ref[3:4] = jnp.broadcast_to(bias, (1, LANES))
    consts_ref[4:5, 0:SEQS] = (lengths_ref[...] + accepted_ref[...]).astype(F32)
    x = x_ref[...].reshape(ROWS, DH).astype(F32)
    scaled = (x * gain_ref[...]).astype(BF16)
    blocks = [dot_nn(scaled, w[...]) for w in (wq_ref, wk_ref, wv_ref)]
    wide = jnp.concatenate([scaled, scaled], axis=1)
    half = (iota((ROWS, LANES), 1) // DH == lax.rem(kv, 2)).astype(F32).astype(BF16)
    gates = dot_nt(wf_ref[...], wide * half)
    own = jnp.where(tp == 0, gates[:HEADS], gates[HEADS:])
    squares = jnp.sum(x * x, axis=1, keepdims=True)
    diagonal = iota((ROWS, LANES), 0) == iota((ROWS, LANES), 1)
    square_row = jnp.sum(jnp.where(diagonal, squares, 0.0), axis=0, keepdims=True)[:, :DH]
    for s in range(SEQS):
        for c in range(QUARTERS):
            query, key, value = (
                packed(
                    *(
                        block[at : at + SUB, LANES * c : LANES * c + LANES]
                        for at in (PROPS * s, PROPS * s + SUB)
                    )
                )
                for block in blocks
            )
            for j in range(2):
                head = 2 * c + j
                peer = s * HEADS + head
                out_ref[SEND_A * peer : SEND_A * peer + SUB, :] = query[j]
                out_ref[SEND_A * peer + SUB : SEND_A * (peer + 1), :] = jnp.concatenate(
                    [own[head : head + 1], square_row], axis=1
                )
                high = key[j].astype(BF16).astype(F32)
                part_ref[peer] = jnp.concatenate([high, key[j] - high, value[j]], axis=0).astype(BF16)


def head_scale(block):
    left = iota(block.shape, 1) < DH
    square = block * block
    first = jnp.sum(jnp.where(left, square, 0.0), axis=1, keepdims=True)
    second = jnp.sum(jnp.where(left, 0.0, square), axis=1, keepdims=True)
    return lax.rsqrt(jnp.where(left, first, second) / DH + EPSILON)


def finish_kernel(got_ref, part_ref, consts_ref, out_ref, row_ref, inverse_ref):
    s = lax.div(lax.axis_index("kv"), HEADS)
    query = got_ref[0:SUB]
    tail = got_ref[SUB:SEND_A]
    for p in range(1, N_KV):
        query = query + got_ref[SEND_A * p : SEND_A * p + SUB]
        tail = tail + got_ref[SEND_A * p + SUB : SEND_A * (p + 1)]
    other = swapped(jnp.broadcast_to(tail, (SUB, LANES)))[0:1]
    left = left_of((1, LANES))
    square = jnp.where(left, other, tail)
    gate_sum = jnp.where(left, tail, other)
    inverse_row = lax.rsqrt(square / (N_KV * DH) + EPSILON)
    lane = iota((SUB, LANES), 1)
    first = iota((SUB, LANES), 0) + s * PROPS
    upper = jnp.sum(jnp.where(lane == first, inverse_row, 0.0), axis=1, keepdims=True)
    lower = jnp.sum(jnp.where(lane == first + SUB, inverse_row, 0.0), axis=1, keepdims=True)
    inverse = jnp.where(left_of((SUB, LANES)), upper, lower)
    inverse_ref[...] = inverse
    query = query * inverse
    query = query * head_scale(query) * consts_ref[0:1]
    logit = gate_sum * inverse_row + consts_ref[3:4]
    small = jnp.exp(-jnp.abs(logit))
    one_more = 1.0 + small
    grown = jnp.where(
        one_more == 1.0, small, jnp.log(one_more) * small / jnp.where(one_more == 1.0, 1.0, one_more - 1.0)
    )
    row_ref[...] = jnp.minimum(logit, 0.0) - grown
    whole = query.astype(BF16)
    for p in range(N_KV):
        out_ref[p, 0:SUB] = whole
        out_ref[p, SUB:SEND_B] = part_ref[p]


def stage_kernel(
    key_hbm, value_hbm, gate_hbm, parents_ref, row_ref,
    key_ref, held_ref, gate_ref, bias_ref, new_key_hbm, new_value_hbm,
    rest_ref, sems,
):
    gate_load = pltpu.make_async_copy(gate_hbm, gate_ref, sems.at[2, 0])
    gate_load.start()
    targets = [key_ref.at[s] for s in range(SEQS)]
    targets += [held_ref.at[s] if s < HELD else rest_ref.at[s - HELD] for s in range(SEQS)]
    sources = [key_hbm.at[s] for s in range(SEQS)] + [value_hbm.at[s] for s in range(SEQS)]
    news = [new_key_hbm.at[s] for s in range(SEQS)] + [new_value_hbm.at[s] for s in range(SEQS)]
    loads = [pltpu.make_async_copy(a, b, sems.at[0, n]) for n, (a, b) in enumerate(zip(sources, targets))]
    stores = [pltpu.make_async_copy(a, b, sems.at[1, n]) for n, (a, b) in enumerate(zip(targets, news))]
    for load in loads:
        load.start()
    bias_ref[...] = tree_bias(parents_ref, row_ref)
    for load, store in zip(loads, stores):
        load.wait()
        store.start()
    gate_load.wait()
    for store in stores:
        store.wait()


def tree_bias(parents_ref, row_ref):
    s = lax.div(lax.axis_index("kv"), HEADS)
    square = (PROPS, PROPS)
    step = (iota(square, 0) == parents_ref[pl.ds(s, 1), :]).astype(F32)
    identity = (iota(square, 0) == iota(square, 1)).astype(F32)
    above = identity + step
    reach = step
    for _ in range(3):
        reach = dot_nn(reach, reach)
        above = above + dot_nn(above, reach)
    wide = (PROPS, LANES)
    wanted = iota(wide, 1) == iota(wide, 0) + s * PROPS
    gate = jnp.sum(jnp.where(wanted, row_ref[...], 0.0), axis=1, keepdims=True)
    path = jnp.sum(above * gate, axis=0, keepdims=True)
    return jnp.where(dot_nt(identity, above) > 0.5, -path, MASKED)


def attend_kernel(
    consts_ref, inverse_ref, row_ref, bias_ref, got_ref, key_ref, held_ref, gate_ref, value_hbm,
    out_ref, tree_ref, own_ref, rest_ref, weights_ref, sems,
):
    loads = {}
    for s in range(HELD, SEQS):
        loads[s] = pltpu.make_async_copy(value_hbm.at[s], rest_ref.at[s - HELD], sems.at[s])
        loads[s].start()
    sums = []
    for s in range(SEQS):
        raw = score_sequence(s, got_ref, key_ref)
        sums.append(weigh_sequence(s, raw, consts_ref[4:5, s : s + 1], gate_ref, weights_ref))
    attend_tree(consts_ref, inverse_ref, bias_ref, got_ref, tree_ref, own_ref)
    tail = row_ref[...]
    for s in range(SEQS):
        if s in loads:
            loads[s].wait()
        values = held_ref[s] if s < HELD else rest_ref[s - HELD]
        send_sequence(s, dot_nn(weights_ref[s], values), *sums[s], tail, out_ref)


def score_sequence(s, got_ref, key_ref):
    query = unpacked_rows(lambda p: got_ref[p, 0:SUB], s)
    wide = (HEADS * PROPS, WIDTH)
    own_head = iota(wide, 0) // PROPS == iota(wide, 1) // DH
    mask = jnp.where(own_head, 0.125, 0.0).astype(BF16)
    spread = jnp.concatenate([query] * HEADS, axis=0) * mask
    return dot_nt(spread, key_ref[s])


def weigh_sequence(s, scores, base, gate_ref, weights_ref):
    kv = lax.axis_index("kv")
    gate = gate_ref[s]
    edge_hit = (iota((HEADS, BLOCK), 1) + (kv * BLOCK + 1)).astype(F32) == base
    edge = jnp.sum(jnp.where(edge_hit, gate, 0.0), axis=1, keepdims=True)
    gates = jnp.concatenate(
        [jnp.broadcast_to(gate[h : h + 1], (PROPS, BLOCK)) for h in range(HEADS)], axis=0
    )
    position = (iota((HEADS * PROPS, BLOCK), 1) + kv * BLOCK).astype(F32)
    live = position < base
    scores = jnp.where(live, scores - gates, MASKED)
    peak = jnp.max(scores, axis=1, keepdims=True)
    weights = jnp.where(live, jnp.exp(scores - peak), 0.0)
    total = jnp.sum(weights, axis=1, keepdims=True)
    weights_ref[s] = weights.astype(BF16)
    some = total > 0.0
    safe = jnp.where(some, total, 1.0)
    log_sum = jnp.where(some, peak + jnp.log(safe), MASKED)
    return 1.0 / safe, log_sum, edge


def send_sequence(s, weighted, scale, log_sum, edge, tail, out_ref):
    weighted = weighted * scale
    lane = iota((PROPS, WIDTH), 1) // DH
    joined = jnp.zeros((PROPS, WIDTH), F32)
    for h in range(HEADS):
        joined = jnp.where(lane == h, weighted[h * PROPS : (h + 1) * PROPS], joined)
    whole = (LANES, LANES)
    spread = jnp.where(iota(whole, 0) == iota(whole, 1), log_sum, 0.0)
    log_row = jnp.sum(spread, axis=0, keepdims=True)
    lane = iota((1, LANES), 1)
    for c in range(QUARTERS):
        part = joined[:, LANES * c : LANES * c + LANES]
        both = packed(part[:SUB], part[SUB:])
        for j in range(2):
            h = 2 * c + j
            at = (s * HEADS + h) * SEND_C
            row = jnp.where(lane // PROPS == h, log_row, edge[h : h + 1])
            row = jnp.where(lane // DH == h // QUARTERS, row, tail)
            out_ref[at : at + SUB, :] = both[j]
            out_ref[at + SUB : at + SEND_C, :] = row


def attend_tree(consts_ref, inverse_ref, bias_ref, got_ref, tree_ref, own_ref):
    key = jnp.zeros((SUB, LANES), F32)
    value = jnp.zeros((SUB, LANES), F32)
    for p in range(N_KV):
        high, low, part = (got_ref[p, SUB * i : SUB * i + SUB].astype(F32) for i in range(1, 4))
        key = key + (high + low)
        value = value + part
    inverse = inverse_ref[...]
    key = key * inverse
    key = (key * head_scale(key) * consts_ref[1:2]).astype(BF16).astype(F32)
    value = (value * inverse).astype(BF16).astype(F32)
    own_ref[...] = jnp.concatenate([key, value], axis=0).astype(BF16)
    query = got_ref[lax.axis_index("kv"), 0:SUB].astype(F32)
    left = left_of((PROPS, LANES))
    query, keys, values = (jnp.concatenate([x, swapped(x)], axis=0) for x in (query, key, value))
    query = jnp.where(left, query, 0.0).astype(BF16)
    bias = bias_ref[...]
    scores = dot_nt(query, keys.astype(BF16)) * 0.125 + bias
    peak = jnp.max(scores, axis=1, keepdims=True)
    weights = jnp.where(bias > 0.5 * MASKED, jnp.exp(scores - peak), 0.0)
    total = jnp.sum(weights, axis=1, keepdims=True)
    weighted = dot_nn(weights.astype(BF16), values.astype(BF16)) / total
    log_sum = peak + jnp.log(total)
    tree_ref[0:SUB] = jnp.where(left[:SUB], weighted[:SUB], swapped(weighted[SUB:]))
    tree_ref[SUB:] = jnp.where(left[:SUB], log_sum[:SUB], log_sum[SUB:])


def merge_kernel(got_ref, tree_ref, own_ref, consts_ref, out_ref):
    h = lax.rem(lax.axis_index("kv"), HEADS)
    shape = (LANES, LANES)
    source = iota(shape, 0)
    same = lax.rem(source, PROPS) // SUB == iota(shape, 1) // DH
    choose = jnp.where((source // PROPS == h) & same, 1.0, 0.0).astype(BF16)
    tile = (SUB, LANES)
    wanted = (iota(tile, 1) // PROPS == h) & (lax.rem(iota(tile, 1), SUB) == iota(tile, 0))
    edge_lane = lax.div(h, QUARTERS) * DH + lax.rem(h + 1, QUARTERS) * PROPS
    rows = [got_ref[SEND_C * p + SUB : SEND_C * (p + 1), :] for p in range(N_KV)]
    edge = rows[0]
    for row in rows[1:]:
        edge = edge + row
    edge = jnp.sum(jnp.where(iota((1, LANES), 1) == edge_lane, edge, 0.0), axis=1, keepdims=True)
    spread = jnp.concatenate([jnp.where(wanted, row, 0.0) for row in rows], axis=0)
    log_sums = jnp.zeros((N_KV * SUB, LANES), F32)
    for piece in pieces(spread):
        log_sums = log_sums + dot_nn(piece.astype(BF16), choose)
    top = log_sums[0:SUB]
    for p in range(1, N_KV):
        top = jnp.maximum(top, log_sums[SUB * p : SUB * p + SUB])
    tree_sum = tree_ref[SUB:] - edge
    top = jnp.maximum(top, tree_sum)
    weight = jnp.exp(tree_sum - top)
    below = weight
    above = weight * tree_ref[0:SUB]
    for p in range(N_KV):
        weight = jnp.exp(log_sums[SUB * p : SUB * p + SUB] - top)
        below = below + weight
        part = got_ref[SEND_C * p : SEND_C * p + SUB, :]
        above = above + weight * part
    attended = above / below
    normed = attended * head_scale(attended) * consts_ref[2:3]
    whole = normed.astype(BF16)
    own = own_ref[...]
    for p in range(N_KV):
        out_ref[p, 0:SUB] = whole
        out_ref[p, SUB:SEND_D] = own


def out_kernel(got_ref, w_ref, out_ref):
    rows = jnp.concatenate([unpacked_rows(lambda p: got_ref[p, 0:SUB], s) for s in range(SEQS)], axis=0)
    result = dot_nt(rows, w_ref[...])
    out_ref[...] = result.astype(BF16)


def write_kernel(
    consts_ref, parts_ref, got_ref, key_hbm, value_hbm, _k, _v,
    new_key_hbm, new_value_hbm, gates_ref, old_ref, rows_ref, sems,
):
    kv = lax.axis_index("kv")
    window = 2 * PROPS
    bases = [jnp.max(consts_ref[4:5, s : s + 1]).astype(jnp.int32) for s in range(SEQS)]
    firsts = [base - kv * BLOCK for base in bases]
    mine = [(first > -PROPS) & (first < BLOCK) for first in firsts]
    starts = [
        pl.multiple_of(jnp.minimum(lax.div(jnp.maximum(first, 0), PROPS) * PROPS, BLOCK - window), PROPS)
        for first in firsts
    ]

    def load(s, i):
        source = (key_hbm, value_hbm)[i].at[s, pl.ds(starts[s], window), :]
        return pltpu.make_async_copy(source, old_ref.at[2 * s + i], sems.at[0, 2 * s + i])

    def store(s, i):
        target = (new_key_hbm, new_value_hbm)[i].at[s, pl.ds(starts[s], window), :]
        return pltpu.make_async_copy(rows_ref.at[2 * s + i], target, sems.at[1, 2 * s + i])

    for s in range(SEQS):

        @pl.when(mine[s])
        def _():
            for i in range(2):
                load(s, i).start()

    for h in range(HEADS):
        row = parts_ref[SEND_C * h + SUB : SEND_C * (h + 1), :]
        row = jnp.where(lax.rem(kv, HEADS) < QUARTERS, row[:, DH:], row[:, :DH])
        for t in range(SEQS):
            at = PROPS * t
            gates_ref[t, h : h + 1, :] = row[:, at : at + PROPS]
    for s in range(SEQS):

        @pl.when(mine[s])
        def _():
            offset = starts[s] - firsts[s]
            placing = (iota((window, PROPS), 0) + offset == iota((window, PROPS), 1)).astype(F32).astype(BF16)
            line = iota((window, WIDTH), 0) + offset
            hit = (line >= 0) & (line < PROPS)
            for i in range(2):
                at = SUB * (i + 1)
                rows = unpacked_rows(lambda p: got_ref[p, at : at + SUB], s)
                written = dot_nn(placing, rows)
                load(s, i).wait()
                old = old_ref[2 * s + i].astype(F32)
                rows_ref[2 * s + i] = jnp.where(hit, written, old).astype(BF16)
                store(s, i).start()

    for s in range(SEQS):

        @pl.when(mine[s])
        def _():
            for i in range(2):
                store(s, i).wait()


def exchange(array):
    return lax.all_to_all(array, "kv", split_axis=0, concat_axis=0, tiled=True)


def shards(
    tokens,
    norm_gain,
    w_query,
    w_key,
    w_value,
    w_forget,
    forget_bias,
    query_gain,
    key_gain,
    head_gain,
    w_out,
    key_cache,
    value_cache,
    gate_cache,
    lengths,
    accepted,
    parents,
):
    def line(gain):
        return gain.reshape(1, DH)

    def limit(size):
        return pltpu.CompilerParams(vmem_limit_bytes=size * 2**20)

    cache = jax.ShapeDtypeStruct(key_cache.shape, BF16)
    sent, part, consts = pl.pallas_call(
        project_kernel,
        out_shape=(
            jax.ShapeDtypeStruct((N_KV * SEND_A, LANES), F32),
            jax.ShapeDtypeStruct((N_KV, SEND_KV, LANES), BF16),
            jax.ShapeDtypeStruct((SUB, LANES), F32),
        ),
        in_specs=[hbm()] * 12,
        out_specs=(vmem(), vmem(), vmem()),
        scratch_shapes=[
            pltpu.VMEM((SEQS, PROPS, DH), BF16),
            pltpu.VMEM((1, DH), F32),
            pltpu.VMEM((DH, WIDTH), BF16),
            pltpu.VMEM((DH, WIDTH), BF16),
            pltpu.VMEM((DH, WIDTH), BF16),
            pltpu.VMEM((2 * HEADS, LANES), BF16),
            pltpu.VMEM((1, DH), F32),
            pltpu.VMEM((1, DH), F32),
            pltpu.VMEM((1, DH), F32),
            pltpu.VMEM((1, 2 * HEADS), F32),
            pltpu.VMEM((1, SEQS), jnp.int32),
            pltpu.VMEM((1, SEQS), jnp.int32),
            pltpu.SemaphoreType.DMA((12,)),
        ],
        cost_estimate=cost(13_000_000, 700_000),
        compiler_params=limit(8),
        name="project",
    )(
        *map(
            stay,
            (
                tokens, line(norm_gain), w_query, w_key, w_value, w_forget.T,
                line(query_gain), line(key_gain), line(head_gain), forget_bias.reshape(1, 2 * HEADS),
                lengths.reshape(1, SEQS), accepted.reshape(1, SEQS),
            ),
        )
    )
    got = exchange(sent.reshape(N_KV, 1, SEND_A * LANES)).reshape(N_KV * SEND_A, LANES)
    sent, gate_row, inverse = pl.pallas_call(
        finish_kernel,
        out_shape=(
            jax.ShapeDtypeStruct((N_KV, SEND_B, LANES), BF16),
            jax.ShapeDtypeStruct((1, LANES), F32),
            jax.ShapeDtypeStruct((SUB, LANES), F32),
        ),
        in_specs=[vmem()] * 3,
        out_specs=(vmem(), vmem(), vmem()),
        cost_estimate=cost(1_000_000, 700_000),
        compiler_params=limit(8),
        name="finish",
    )(got, part, consts)
    rows = exchange(sent)
    gate_row, key_cache, value_cache, gate_cache = lax.optimization_barrier(
        (gate_row, key_cache, value_cache, gate_cache)
    )
    keys, held, gate_block, bias, new_keys, new_values = pl.pallas_call(
        stage_kernel,
        out_shape=(
            cache,
            jax.ShapeDtypeStruct((HELD, BLOCK, WIDTH), BF16),
            jax.ShapeDtypeStruct(gate_cache.shape, F32),
            jax.ShapeDtypeStruct((PROPS, PROPS), F32),
            pltpu.HBM(key_cache.shape, BF16),
            pltpu.HBM(value_cache.shape, BF16),
        ),
        in_specs=[hbm()] * 3 + [vmem()] * 2,
        out_specs=(vmem(),) * 4 + (hbm(), hbm()),
        scratch_shapes=[
            pltpu.VMEM((SEQS - HELD, BLOCK, WIDTH), BF16),
            pltpu.SemaphoreType.DMA((3, 2 * SEQS)),
        ],
        cost_estimate=cost(500_000_000, 8_500_000),
        compiler_params=limit(8),
        name="stage",
    )(stay(key_cache), stay(value_cache), stay(gate_cache), parents, gate_row)
    rows, keys, held, gate_block = lax.optimization_barrier((rows, keys, held, gate_block))
    sent, tree, own = pl.pallas_call(
        attend_kernel,
        out_shape=(
            jax.ShapeDtypeStruct((N_KV * SEND_C, LANES), F32),
            jax.ShapeDtypeStruct((2 * SUB, LANES), F32),
            jax.ShapeDtypeStruct((2 * SUB, LANES), BF16),
        ),
        in_specs=[vmem()] * 8 + [hbm()],
        out_specs=(vmem(), vmem(), vmem()),
        scratch_shapes=[
            pltpu.VMEM((SEQS - HELD, BLOCK, WIDTH), BF16),
            pltpu.VMEM((SEQS, HEADS * PROPS, BLOCK), BF16),
            pltpu.SemaphoreType.DMA((SEQS + 1,)),
        ],
        cost_estimate=cost(600_000_000, 4_500_000),
        compiler_params=limit(16),
        name="attend",
    )(consts, inverse, gate_row, bias, rows, keys, held, gate_block, stay(value_cache))
    parts = exchange(sent.reshape(N_KV, 1, SEND_C * LANES)).reshape(N_KV * SEND_C, LANES)
    sent = pl.pallas_call(
        merge_kernel,
        out_shape=jax.ShapeDtypeStruct((N_KV, SEND_D, LANES), BF16),
        in_specs=[vmem()] * 4,
        out_specs=vmem(),
        cost_estimate=cost(8_000_000, 200_000),
        compiler_params=limit(8),
        name="merge",
    )(parts, tree, own, consts)
    normed = exchange(sent)
    term = pl.pallas_call(
        out_kernel,
        out_shape=jax.ShapeDtypeStruct((ROWS, DH), BF16),
        in_specs=[vmem()] * 2,
        out_specs=vmem(),
        cost_estimate=cost(4_000_000, 150_000),
        compiler_params=limit(8),
        name="out",
    )(normed, w_out.T)
    other = lax.ppermute(term, "tp", [(0, 1), (1, 0)])
    term, parts = lax.optimization_barrier((term, parts))
    new_keys, new_values, gates = pl.pallas_call(
        write_kernel,
        out_shape=(cache, cache, jax.ShapeDtypeStruct((SEQS, HEADS, PROPS), F32)),
        in_specs=[vmem()] * 3 + [hbm()] * 4,
        out_specs=(hbm(), hbm(), vmem()),
        scratch_shapes=[
            pltpu.VMEM((2 * SEQS, 2 * PROPS, WIDTH), BF16),
            pltpu.VMEM((2 * SEQS, 2 * PROPS, WIDTH), BF16),
            pltpu.SemaphoreType.DMA((2, 2 * SEQS)),
        ],
        input_output_aliases={5: 0, 6: 1},
        cost_estimate=cost(60_000_000, 1_000_000),
        compiler_params=limit(8),
        name="write",
    )(
        consts, parts, normed, stay(key_cache), stay(value_cache), stay(new_keys), stay(new_values)
    )
    layer_out = (term.astype(F32) + other.astype(F32)).astype(BF16)
    return (layer_out.reshape(SEQS, PROPS, DH), new_keys, new_values, gates.transpose(0, 2, 1))


def solution(mesh):
    placed = (
        P("dp", None, "kv"),
        P("kv"),
        P("kv", "tp"),
        P("kv", "tp"),
        P("kv", "tp"),
        P(),
        P(),
        P(),
        P(),
        P(),
        P("tp", "kv"),
        P("dp", "kv", "tp"),
        P("dp", "kv", "tp"),
        P("dp", "tp", "kv"),
        P("dp"),
        P("dp"),
        P("dp", None),
    )
    return jax.shard_map(
        shards,
        mesh=mesh,
        in_specs=placed,
        out_specs=(
            P("dp", None, "kv"),
            P("dp", "kv", "tp"),
            P("dp", "kv", "tp"),
            P("dp", None, "tp"),
        ),
        check_vma=False,
    )
```

```python
import jax
import jax.numpy as jnp
from jax import lax
from jax.experimental import pallas as pl
from jax.experimental.pallas import tpu as pltpu
from jax.sharding import PartitionSpec as P

EPSILON = 1e-06
MASKED = -1e30
F32 = jnp.float32
BF16 = jnp.bfloat16

LANES = 128
SUB = 8
N_KV = 32
QUARTERS = 4
ROWS = 64
HEADS = 8
DH = 64
WIDTH = 512
PROPS = 16
SEQS = 4
BLOCK = 512
SEND_A = 9
SEND_KV = 24
SEND_B = SUB + SEND_KV
SEND_C = 9
SEND_D = 24
HELD = 2


def iota(shape, dim):
    return lax.broadcasted_iota(jnp.int32, shape, dim)


def dot_nn(a, b):
    return lax.dot_general(a, b, (((1,), (0,)), ((), ())), preferred_element_type=F32)


def dot_nt(a, b):
    return lax.dot_general(a, b, (((1,), (1,)), ((), ())), preferred_element_type=F32)


def pieces(x):
    high = x.astype(BF16).astype(F32)
    rest = x - high
    middle = rest.astype(BF16).astype(F32)
    return high, middle, rest - middle


def left_of(shape):
    return iota(shape, len(shape) - 1) < DH


def swapped(block):
    return pltpu.roll(block, DH, 1)


def packed(top, bottom):
    left = left_of(top.shape)
    return jnp.where(left, top, swapped(bottom)), jnp.where(left, swapped(top), bottom)


def unpacked_rows(read, s):
    tiles = []
    for c in range(QUARTERS):
        even, odd = (read(s * HEADS + 2 * c + j).astype(F32) for j in range(2))
        tiles.append(jnp.concatenate(packed(even, odd), axis=0))
    return jnp.concatenate(tiles, axis=1).astype(BF16)


def vmem():
    return pl.BlockSpec(memory_space=pltpu.VMEM)


def stay(array):
    return pltpu.with_memory_space_constraint(array, pltpu.HBM)


def hbm():
    return pl.BlockSpec(memory_space=pltpu.HBM)


def cost(flops, moved):
    return pl.CostEstimate(flops=flops, bytes_accessed=moved, transcendentals=0)


def doubled(gain_ref):
    gain = gain_ref[...]
    return jnp.concatenate([gain, gain], axis=1)


def project_kernel(
    x_hbm, gain_hbm, wq_hbm, wk_hbm, wv_hbm, wf_hbm, qgain_hbm, kgain_hbm, hgain_hbm, bias_hbm, lengths_hbm, accepted_hbm,
    out_ref, part_ref, consts_ref,
    x_ref, gain_ref, wq_ref, wk_ref, wv_ref, wf_ref, qgain_ref, kgain_ref, hgain_ref, bias_ref, lengths_ref, accepted_ref, sems,
):
    kv = lax.axis_index("kv")
    tp = lax.axis_index("tp")
    column = pl.multiple_of(lax.div(kv, 2) * LANES, LANES)
    pairs = (
        (x_hbm, x_ref),
        (gain_hbm, gain_ref),
        (wq_hbm, wq_ref),
        (wk_hbm, wk_ref),
        (wv_hbm, wv_ref),
        (wf_hbm.at[:, pl.ds(column, LANES)], wf_ref),
        (qgain_hbm, qgain_ref),
        (kgain_hbm, kgain_ref),
        (hgain_hbm, hgain_ref),
        (bias_hbm, bias_ref),
        (lengths_hbm, lengths_ref),
        (accepted_hbm, accepted_ref),
    )
    copies = [pltpu.make_async_copy(a, b, sems.at[n]) for n, (a, b) in enumerate(pairs)]
    for copy in copies:
        copy.start()
    for copy in copies:
        copy.wait()
    at = tp * HEADS + lax.rem(kv, HEADS)
    spot = iota((1, 2 * HEADS), 1)
    bias = jnp.sum(jnp.where(spot == at, bias_ref[...], 0.0), axis=1, keepdims=True)
    consts_ref[0:1] = doubled(qgain_ref)
    consts_ref[1:2] = doubled(kgain_ref)
    consts_ref[2:3] = doubled(hgain_ref)
    consts_ref[3:4] = jnp.broadcast_to(bias, (1, LANES))
    consts_ref[4:5, 0:SEQS] = (lengths_ref[...] + accepted_ref[...]).astype(F32)
    x = x_ref[...].reshape(ROWS, DH).astype(F32)
    scaled = (x * gain_ref[...]).astype(BF16)
    blocks = [dot_nn(scaled, w[...]) for w in (wq_ref, wk_ref, wv_ref)]
    wide = jnp.concatenate([scaled, scaled], axis=1)
    half = (iota((ROWS, LANES), 1) // DH == lax.rem(kv, 2)).astype(F32).astype(BF16)
    gates = dot_nt(wf_ref[...], wide * half)
    own = jnp.where(tp == 0, gates[:HEADS], gates[HEADS:])
    squares = jnp.sum(x * x, axis=1, keepdims=True)
    diagonal = iota((ROWS, LANES), 0) == iota((ROWS, LANES), 1)
    square_row = jnp.sum(jnp.where(diagonal, squares, 0.0), axis=0, keepdims=True)[:, :DH]
    for s in range(SEQS):
        for c in range(QUARTERS):
            query, key, value = (
                packed(
                    *(
                        block[at : at + SUB, LANES * c : LANES * c + LANES]
                        for at in (PROPS * s, PROPS * s + SUB)
                    )
                )
                for block in blocks
            )
            for j in range(2):
                head = 2 * c + j
                peer = s * HEADS + head
                out_ref[SEND_A * peer : SEND_A * peer + SUB, :] = query[j]
                out_ref[SEND_A * peer + SUB : SEND_A * (peer + 1), :] = jnp.concatenate(
                    [own[head : head + 1], square_row], axis=1
                )
                high = key[j].astype(BF16).astype(F32)
                part_ref[peer] = jnp.concatenate([high, key[j] - high, value[j]], axis=0).astype(BF16)


def head_scale(block):
    left = iota(block.shape, 1) < DH
    square = block * block
    first = jnp.sum(jnp.where(left, square, 0.0), axis=1, keepdims=True)
    second = jnp.sum(jnp.where(left, 0.0, square), axis=1, keepdims=True)
    return lax.rsqrt(jnp.where(left, first, second) / DH + EPSILON)


def finish_kernel(got_ref, part_ref, consts_ref, out_ref, row_ref, inverse_ref):
    s = lax.div(lax.axis_index("kv"), HEADS)
    query = got_ref[0:SUB]
    tail = got_ref[SUB:SEND_A]
    for p in range(1, N_KV):
        query = query + got_ref[SEND_A * p : SEND_A * p + SUB]
        tail = tail + got_ref[SEND_A * p + SUB : SEND_A * (p + 1)]
    other = swapped(jnp.broadcast_to(tail, (SUB, LANES)))[0:1]
    left = left_of((1, LANES))
    square = jnp.where(left, other, tail)
    gate_sum = jnp.where(left, tail, other)
    inverse_row = lax.rsqrt(square / (N_KV * DH) + EPSILON)
    lane = iota((SUB, LANES), 1)
    first = iota((SUB, LANES), 0) + s * PROPS
    upper = jnp.sum(jnp.where(lane == first, inverse_row, 0.0), axis=1, keepdims=True)
    lower = jnp.sum(jnp.where(lane == first + SUB, inverse_row, 0.0), axis=1, keepdims=True)
    inverse = jnp.where(left_of((SUB, LANES)), upper, lower)
    inverse_ref[...] = inverse
    query = query * inverse
    query = query * head_scale(query) * consts_ref[0:1]
    logit = gate_sum * inverse_row + consts_ref[3:4]
    small = jnp.exp(-jnp.abs(logit))
    one_more = 1.0 + small
    grown = jnp.where(
        one_more == 1.0, small, jnp.log(one_more) * small / jnp.where(one_more == 1.0, 1.0, one_more - 1.0)
    )
    row_ref[...] = jnp.minimum(logit, 0.0) - grown
    whole = query.astype(BF16)
    for p in range(N_KV):
        out_ref[p, 0:SUB] = whole
        out_ref[p, SUB:SEND_B] = part_ref[p]


def stage_kernel(
    key_hbm, value_hbm, gate_hbm, parents_ref, row_ref,
    key_ref, held_ref, gate_ref, bias_ref, new_key_hbm, new_value_hbm,
    rest_ref, sems,
):
    gate_load = pltpu.make_async_copy(gate_hbm, gate_ref, sems.at[2, 0])
    gate_load.start()
    targets = [key_ref.at[s] for s in range(SEQS)]
    targets += [held_ref.at[s] if s < HELD else rest_ref.at[s - HELD] for s in range(SEQS)]
    sources = [key_hbm.at[s] for s in range(SEQS)] + [value_hbm.at[s] for s in range(SEQS)]
    news = [new_key_hbm.at[s] for s in range(SEQS)] + [new_value_hbm.at[s] for s in range(SEQS)]
    loads = [pltpu.make_async_copy(a, b, sems.at[0, n]) for n, (a, b) in enumerate(zip(sources, targets))]
    stores = [pltpu.make_async_copy(a, b, sems.at[1, n]) for n, (a, b) in enumerate(zip(targets, news))]
    for load in loads:
        load.start()
    bias_ref[...] = tree_bias(parents_ref, row_ref)
    for load, store in zip(loads, stores):
        load.wait()
        store.start()
    gate_load.wait()
    for store in stores:
        store.wait()


def tree_bias(parents_ref, row_ref):
    s = lax.div(lax.axis_index("kv"), HEADS)
    square = (PROPS, PROPS)
    step = (iota(square, 0) == parents_ref[pl.ds(s, 1), :]).astype(F32)
    identity = (iota(square, 0) == iota(square, 1)).astype(F32)
    above = identity + step
    reach = step
    for _ in range(3):
        reach = dot_nn(reach, reach)
        above = above + dot_nn(above, reach)
    wide = (PROPS, LANES)
    wanted = iota(wide, 1) == iota(wide, 0) + s * PROPS
    gate = jnp.sum(jnp.where(wanted, row_ref[...], 0.0), axis=1, keepdims=True)
    path = jnp.sum(above * gate, axis=0, keepdims=True)
    return jnp.where(dot_nt(identity, above) > 0.5, -path, MASKED)


def attend_kernel(
    consts_ref, inverse_ref, row_ref, bias_ref, got_ref, key_ref, held_ref, gate_ref, value_hbm,
    out_ref, tree_ref, own_ref, rest_ref, weights_ref, sems,
):
    loads = {
        s: pltpu.make_async_copy(value_hbm.at[s], rest_ref.at[s - HELD], sems.at[s])
        for s in range(HELD, SEQS)
    }

    @pl.loop(HELD, SEQS)
    def _(s):
        pltpu.make_async_copy(value_hbm.at[s], rest_ref.at[s - HELD], sems.at[s]).start()

    sums = []
    for s in range(SEQS):
        raw = score_sequence(s, got_ref, key_ref)
        sums.append(weigh_sequence(s, raw, consts_ref[4:5, s : s + 1], gate_ref, weights_ref))
    attend_tree(consts_ref, inverse_ref, bias_ref, got_ref, tree_ref, own_ref)
    tail = row_ref[...]
    for s in range(SEQS):
        if s in loads:
            loads[s].wait()
        values = held_ref[s] if s < HELD else rest_ref[s - HELD]
        send_sequence(s, dot_nn(weights_ref[s], values), *sums[s], tail, out_ref)


def score_sequence(s, got_ref, key_ref):
    query = unpacked_rows(lambda p: got_ref[p, 0:SUB], s)
    wide = (HEADS * PROPS, WIDTH)
    own_head = iota(wide, 0) // PROPS == iota(wide, 1) // DH
    mask = jnp.where(own_head, 0.125, 0.0).astype(BF16)
    spread = jnp.concatenate([query] * HEADS, axis=0) * mask
    return dot_nt(spread, key_ref[s])


def weigh_sequence(s, scores, base, gate_ref, weights_ref):
    kv = lax.axis_index("kv")
    gate = gate_ref[s]
    edge_hit = (iota((HEADS, BLOCK), 1) + (kv * BLOCK + 1)).astype(F32) == base
    edge = jnp.sum(jnp.where(edge_hit, gate, 0.0), axis=1, keepdims=True)
    gates = jnp.concatenate(
        [jnp.broadcast_to(gate[h : h + 1], (PROPS, BLOCK)) for h in range(HEADS)], axis=0
    )
    position = (iota((HEADS * PROPS, BLOCK), 1) + kv * BLOCK).astype(F32)
    live = position < base
    scores = jnp.where(live, scores - gates, MASKED)
    peak = jnp.max(scores, axis=1, keepdims=True)
    weights = jnp.where(live, jnp.exp(scores - peak), 0.0)
    total = jnp.sum(weights, axis=1, keepdims=True)
    weights_ref[s] = weights.astype(BF16)
    some = total > 0.0
    safe = jnp.where(some, total, 1.0)
    log_sum = jnp.where(some, peak + jnp.log(safe), MASKED)
    return 1.0 / safe, log_sum, edge


def send_sequence(s, weighted, scale, log_sum, edge, tail, out_ref):
    weighted = weighted * scale
    lane = iota((PROPS, WIDTH), 1) // DH
    joined = jnp.zeros((PROPS, WIDTH), F32)
    for h in range(HEADS):
        joined = jnp.where(lane == h, weighted[h * PROPS : (h + 1) * PROPS], joined)
    whole = (LANES, LANES)
    spread = jnp.where(iota(whole, 0) == iota(whole, 1), log_sum, 0.0)
    log_row = jnp.sum(spread, axis=0, keepdims=True)
    lane = iota((1, LANES), 1)
    for c in range(QUARTERS):
        part = joined[:, LANES * c : LANES * c + LANES]
        both = packed(part[:SUB], part[SUB:])
        for j in range(2):
            h = 2 * c + j
            at = (s * HEADS + h) * SEND_C
            row = jnp.where(lane // PROPS == h, log_row, edge[h : h + 1])
            row = jnp.where(lane // DH == h // QUARTERS, row, tail)
            out_ref[at : at + SUB, :] = both[j]
            out_ref[at + SUB : at + SEND_C, :] = row


def attend_tree(consts_ref, inverse_ref, bias_ref, got_ref, tree_ref, own_ref):
    key = jnp.zeros((SUB, LANES), F32)
    value = jnp.zeros((SUB, LANES), F32)
    for p in range(N_KV):
        high, low, part = (got_ref[p, SUB * i : SUB * i + SUB].astype(F32) for i in range(1, 4))
        key = key + (high + low)
        value = value + part
    inverse = inverse_ref[...]
    key = key * inverse
    key = (key * head_scale(key) * consts_ref[1:2]).astype(BF16).astype(F32)
    value = (value * inverse).astype(BF16).astype(F32)
    own_ref[...] = jnp.concatenate([key, value], axis=0).astype(BF16)
    query = got_ref[lax.axis_index("kv"), 0:SUB].astype(F32)
    left = left_of((PROPS, LANES))
    query, keys, values = (jnp.concatenate([x, swapped(x)], axis=0) for x in (query, key, value))
    query = jnp.where(left, query, 0.0).astype(BF16)
    bias = bias_ref[...]
    scores = dot_nt(query, keys.astype(BF16)) * 0.125 + bias
    peak = jnp.max(scores, axis=1, keepdims=True)
    weights = jnp.where(bias > 0.5 * MASKED, jnp.exp(scores - peak), 0.0)
    total = jnp.sum(weights, axis=1, keepdims=True)
    weighted = dot_nn(weights.astype(BF16), values.astype(BF16)) / total
    log_sum = peak + jnp.log(total)
    tree_ref[0:SUB] = jnp.where(left[:SUB], weighted[:SUB], swapped(weighted[SUB:]))
    tree_ref[SUB:] = jnp.where(left[:SUB], log_sum[:SUB], log_sum[SUB:])


def merge_kernel(got_ref, tree_ref, own_ref, consts_ref, out_ref):
    h = lax.rem(lax.axis_index("kv"), HEADS)
    shape = (LANES, LANES)
    source = iota(shape, 0)
    same = lax.rem(source, PROPS) // SUB == iota(shape, 1) // DH
    choose = jnp.where((source // PROPS == h) & same, 1.0, 0.0).astype(BF16)
    tile = (SUB, LANES)
    wanted = (iota(tile, 1) // PROPS == h) & (lax.rem(iota(tile, 1), SUB) == iota(tile, 0))
    edge_lane = lax.div(h, QUARTERS) * DH + lax.rem(h + 1, QUARTERS) * PROPS
    rows = [got_ref[SEND_C * p + SUB : SEND_C * (p + 1), :] for p in range(N_KV)]
    edge = rows[0]
    for row in rows[1:]:
        edge = edge + row
    edge = jnp.sum(jnp.where(iota((1, LANES), 1) == edge_lane, edge, 0.0), axis=1, keepdims=True)
    spread = jnp.concatenate([jnp.where(wanted, row, 0.0) for row in rows], axis=0)
    log_sums = jnp.zeros((N_KV * SUB, LANES), F32)
    for piece in pieces(spread):
        log_sums = log_sums + dot_nn(piece.astype(BF16), choose)
    top = log_sums[0:SUB]
    for p in range(1, N_KV):
        top = jnp.maximum(top, log_sums[SUB * p : SUB * p + SUB])
    tree_sum = tree_ref[SUB:] - edge
    top = jnp.maximum(top, tree_sum)
    weight = jnp.exp(tree_sum - top)
    below = weight
    above = weight * tree_ref[0:SUB]
    for p in range(N_KV):
        weight = jnp.exp(log_sums[SUB * p : SUB * p + SUB] - top)
        below = below + weight
        part = got_ref[SEND_C * p : SEND_C * p + SUB, :]
        above = above + weight * part
    attended = above / below
    normed = attended * head_scale(attended) * consts_ref[2:3]
    whole = normed.astype(BF16)
    own = own_ref[...]
    for p in range(N_KV):
        out_ref[p, 0:SUB] = whole
        out_ref[p, SUB:SEND_D] = own


def out_kernel(got_ref, w_ref, out_ref):
    rows = jnp.concatenate([unpacked_rows(lambda p: got_ref[p, 0:SUB], s) for s in range(SEQS)], axis=0)
    result = dot_nt(rows, w_ref[...])
    out_ref[...] = result.astype(BF16)


def write_kernel(
    consts_ref, parts_ref, got_ref, key_hbm, value_hbm, _k, _v,
    new_key_hbm, new_value_hbm, gates_ref, old_ref, rows_ref, sems,
):
    kv = lax.axis_index("kv")
    window = 2 * PROPS
    bases = [jnp.max(consts_ref[4:5, s : s + 1]).astype(jnp.int32) for s in range(SEQS)]
    firsts = [base - kv * BLOCK for base in bases]
    mine = [(first > -PROPS) & (first < BLOCK) for first in firsts]
    starts = [
        pl.multiple_of(jnp.minimum(lax.div(jnp.maximum(first, 0), PROPS) * PROPS, BLOCK - window), PROPS)
        for first in firsts
    ]

    def load(s, i):
        source = (key_hbm, value_hbm)[i].at[s, pl.ds(starts[s], window), :]
        return pltpu.make_async_copy(source, old_ref.at[2 * s + i], sems.at[0, 2 * s + i])

    def store(s, i):
        target = (new_key_hbm, new_value_hbm)[i].at[s, pl.ds(starts[s], window), :]
        return pltpu.make_async_copy(rows_ref.at[2 * s + i], target, sems.at[1, 2 * s + i])

    for s in range(SEQS):

        @pl.when(mine[s])
        def _():
            for i in range(2):
                load(s, i).start()

    for h in range(HEADS):
        row = parts_ref[SEND_C * h + SUB : SEND_C * (h + 1), :]
        row = jnp.where(lax.rem(kv, HEADS) < QUARTERS, row[:, DH:], row[:, :DH])
        for t in range(SEQS):
            at = PROPS * t
            gates_ref[t, h : h + 1, :] = row[:, at : at + PROPS]
    for s in range(SEQS):

        @pl.when(mine[s])
        def _():
            offset = starts[s] - firsts[s]
            placing = (iota((window, PROPS), 0) + offset == iota((window, PROPS), 1)).astype(F32).astype(BF16)
            line = iota((window, WIDTH), 0) + offset
            hit = (line >= 0) & (line < PROPS)
            for i in range(2):
                at = SUB * (i + 1)
                rows = unpacked_rows(lambda p: got_ref[p, at : at + SUB], s)
                written = dot_nn(placing, rows)
                load(s, i).wait()
                old = old_ref[2 * s + i].astype(F32)
                rows_ref[2 * s + i] = jnp.where(hit, written, old).astype(BF16)
                store(s, i).start()

    for s in range(SEQS):

        @pl.when(mine[s])
        def _():
            for i in range(2):
                store(s, i).wait()


def exchange(array):
    return lax.all_to_all(array, "kv", split_axis=0, concat_axis=0, tiled=True)


def shards(
    tokens,
    norm_gain,
    w_query,
    w_key,
    w_value,
    w_forget,
    forget_bias,
    query_gain,
    key_gain,
    head_gain,
    w_out,
    key_cache,
    value_cache,
    gate_cache,
    lengths,
    accepted,
    parents,
):
    def line(gain):
        return gain.reshape(1, DH)

    def limit(size):
        return pltpu.CompilerParams(vmem_limit_bytes=size * 2**20)

    cache = jax.ShapeDtypeStruct(key_cache.shape, BF16)
    sent, part, consts = pl.pallas_call(
        project_kernel,
        out_shape=(
            jax.ShapeDtypeStruct((N_KV * SEND_A, LANES), F32),
            jax.ShapeDtypeStruct((N_KV, SEND_KV, LANES), BF16),
            jax.ShapeDtypeStruct((SUB, LANES), F32),
        ),
        in_specs=[hbm()] * 12,
        out_specs=(vmem(), vmem(), vmem()),
        scratch_shapes=[
            pltpu.VMEM((SEQS, PROPS, DH), BF16),
            pltpu.VMEM((1, DH), F32),
            pltpu.VMEM((DH, WIDTH), BF16),
            pltpu.VMEM((DH, WIDTH), BF16),
            pltpu.VMEM((DH, WIDTH), BF16),
            pltpu.VMEM((2 * HEADS, LANES), BF16),
            pltpu.VMEM((1, DH), F32),
            pltpu.VMEM((1, DH), F32),
            pltpu.VMEM((1, DH), F32),
            pltpu.VMEM((1, 2 * HEADS), F32),
            pltpu.VMEM((1, SEQS), jnp.int32),
            pltpu.VMEM((1, SEQS), jnp.int32),
            pltpu.SemaphoreType.DMA((12,)),
        ],
        cost_estimate=cost(13_000_000, 700_000),
        compiler_params=limit(8),
        name="project",
    )(
        *map(
            stay,
            (
                tokens, line(norm_gain), w_query, w_key, w_value, w_forget.T,
                line(query_gain), line(key_gain), line(head_gain), forget_bias.reshape(1, 2 * HEADS),
                lengths.reshape(1, SEQS), accepted.reshape(1, SEQS),
            ),
        )
    )
    got = exchange(sent.reshape(N_KV, 1, SEND_A * LANES)).reshape(N_KV * SEND_A, LANES)
    sent, gate_row, inverse = pl.pallas_call(
        finish_kernel,
        out_shape=(
            jax.ShapeDtypeStruct((N_KV, SEND_B, LANES), BF16),
            jax.ShapeDtypeStruct((1, LANES), F32),
            jax.ShapeDtypeStruct((SUB, LANES), F32),
        ),
        in_specs=[vmem()] * 3,
        out_specs=(vmem(), vmem(), vmem()),
        cost_estimate=cost(1_000_000, 700_000),
        compiler_params=limit(8),
        name="finish",
    )(got, part, consts)
    rows = exchange(sent)
    gate_row, key_cache, value_cache, gate_cache = lax.optimization_barrier(
        (gate_row, key_cache, value_cache, gate_cache)
    )
    keys, held, gate_block, bias, new_keys, new_values = pl.pallas_call(
        stage_kernel,
        out_shape=(
            cache,
            jax.ShapeDtypeStruct((HELD, BLOCK, WIDTH), BF16),
            jax.ShapeDtypeStruct(gate_cache.shape, F32),
            jax.ShapeDtypeStruct((PROPS, PROPS), F32),
            pltpu.HBM(key_cache.shape, BF16),
            pltpu.HBM(value_cache.shape, BF16),
        ),
        in_specs=[hbm()] * 3 + [vmem()] * 2,
        out_specs=(vmem(),) * 4 + (hbm(), hbm()),
        scratch_shapes=[
            pltpu.VMEM((SEQS - HELD, BLOCK, WIDTH), BF16),
            pltpu.SemaphoreType.DMA((3, 2 * SEQS)),
        ],
        cost_estimate=cost(500_000_000, 8_500_000),
        compiler_params=limit(8),
        name="stage",
    )(stay(key_cache), stay(value_cache), stay(gate_cache), parents, gate_row)
    rows, keys, held, gate_block = lax.optimization_barrier((rows, keys, held, gate_block))
    sent, tree, own = pl.pallas_call(
        attend_kernel,
        out_shape=(
            jax.ShapeDtypeStruct((N_KV * SEND_C, LANES), F32),
            jax.ShapeDtypeStruct((2 * SUB, LANES), F32),
            jax.ShapeDtypeStruct((2 * SUB, LANES), BF16),
        ),
        in_specs=[vmem()] * 8 + [hbm()],
        out_specs=(vmem(), vmem(), vmem()),
        scratch_shapes=[
            pltpu.VMEM((SEQS - HELD, BLOCK, WIDTH), BF16),
            pltpu.VMEM((SEQS, HEADS * PROPS, BLOCK), BF16),
            pltpu.SemaphoreType.DMA((SEQS + 1,)),
        ],
        cost_estimate=cost(600_000_000, 4_500_000),
        compiler_params=limit(16),
        name="attend",
    )(consts, inverse, gate_row, bias, rows, keys, held, gate_block, stay(value_cache))
    parts = exchange(sent.reshape(N_KV, 1, SEND_C * LANES)).reshape(N_KV * SEND_C, LANES)
    sent = pl.pallas_call(
        merge_kernel,
        out_shape=jax.ShapeDtypeStruct((N_KV, SEND_D, LANES), BF16),
        in_specs=[vmem()] * 4,
        out_specs=vmem(),
        cost_estimate=cost(8_000_000, 200_000),
        compiler_params=limit(8),
        name="merge",
    )(parts, tree, own, consts)
    normed = exchange(sent)
    term = pl.pallas_call(
        out_kernel,
        out_shape=jax.ShapeDtypeStruct((ROWS, DH), BF16),
        in_specs=[vmem()] * 2,
        out_specs=vmem(),
        cost_estimate=cost(4_000_000, 150_000),
        compiler_params=limit(8),
        name="out",
    )(normed, w_out.T)
    other = lax.ppermute(term, "tp", [(0, 1), (1, 0)])
    term, parts = lax.optimization_barrier((term, parts))
    new_keys, new_values, gates = pl.pallas_call(
        write_kernel,
        out_shape=(cache, cache, jax.ShapeDtypeStruct((SEQS, HEADS, PROPS), F32)),
        in_specs=[vmem()] * 3 + [hbm()] * 4,
        out_specs=(hbm(), hbm(), vmem()),
        scratch_shapes=[
            pltpu.VMEM((2 * SEQS, 2 * PROPS, WIDTH), BF16),
            pltpu.VMEM((2 * SEQS, 2 * PROPS, WIDTH), BF16),
            pltpu.SemaphoreType.DMA((2, 2 * SEQS)),
        ],
        input_output_aliases={5: 0, 6: 1},
        cost_estimate=cost(60_000_000, 1_000_000),
        compiler_params=limit(8),
        name="write",
    )(
        consts, parts, normed, stay(key_cache), stay(value_cache), stay(new_keys), stay(new_values)
    )
    layer_out = (term.astype(F32) + other.astype(F32)).astype(BF16)
    return (layer_out.reshape(SEQS, PROPS, DH), new_keys, new_values, gates.transpose(0, 2, 1))


def solution(mesh):
    placed = (
        P("dp", None, "kv"),
        P("kv"),
        P("kv", "tp"),
        P("kv", "tp"),
        P("kv", "tp"),
        P(),
        P(),
        P(),
        P(),
        P(),
        P("tp", "kv"),
        P("dp", "kv", "tp"),
        P("dp", "kv", "tp"),
        P("dp", "tp", "kv"),
        P("dp"),
        P("dp"),
        P("dp", None),
    )
    return jax.shard_map(
        shards,
        mesh=mesh,
        in_specs=placed,
        out_specs=(
            P("dp", None, "kv"),
            P("dp", "kv", "tp"),
            P("dp", "kv", "tp"),
            P("dp", None, "tp"),
        ),
        check_vma=False,
    )
```

```python
import jax
import jax.numpy as jnp
from jax import lax
from jax.experimental import pallas as pl
from jax.experimental.pallas import tpu as pltpu
from jax.sharding import PartitionSpec as P

EPSILON = 1e-06
MASKED = -1e30
F32 = jnp.float32
BF16 = jnp.bfloat16

LANES = 128
SUB = 8
N_KV = 32
QUARTERS = 4
ROWS = 64
HEADS = 8
DH = 64
WIDTH = 512
PROPS = 16
SEQS = 4
BLOCK = 512
SEND_A = 9
SEND_KV = 32
SEND_B = SUB + SEND_KV
SEND_C = 9
SEND_D = 24
HELD = 1


def iota(shape, dim):
    return lax.broadcasted_iota(jnp.int32, shape, dim)


def dot_nn(a, b):
    return lax.dot_general(a, b, (((1,), (0,)), ((), ())), preferred_element_type=F32)


def dot_nt(a, b):
    return lax.dot_general(a, b, (((1,), (1,)), ((), ())), preferred_element_type=F32)


def pieces(x):
    high = x.astype(BF16).astype(F32)
    rest = x - high
    middle = rest.astype(BF16).astype(F32)
    return high, middle, rest - middle


def left_of(shape):
    return iota(shape, len(shape) - 1) < DH


def swapped(block):
    return pltpu.roll(block, DH, 1)


def packed(top, bottom):
    left = left_of(top.shape)
    return jnp.where(left, top, swapped(bottom)), jnp.where(left, swapped(top), bottom)


def unpacked_rows(read, s):
    tiles = []
    for c in range(QUARTERS):
        even, odd = (read(s * HEADS + 2 * c + j).astype(F32) for j in range(2))
        tiles.append(jnp.concatenate(packed(even, odd), axis=0))
    return jnp.concatenate(tiles, axis=1).astype(BF16)


def vmem():
    return pl.BlockSpec(memory_space=pltpu.VMEM)


def stay(array):
    return pltpu.with_memory_space_constraint(array, pltpu.HBM)


def hbm():
    return pl.BlockSpec(memory_space=pltpu.HBM)


def cost(flops, moved):
    return pl.CostEstimate(flops=flops, bytes_accessed=moved, transcendentals=0)


def doubled(gain_ref):
    gain = gain_ref[...]
    return jnp.concatenate([gain, gain], axis=1)


def project_kernel(
    x_hbm, gain_hbm, wq_hbm, wk_hbm, wv_hbm, wf_hbm, qgain_hbm, kgain_hbm, hgain_hbm, bias_hbm, lengths_hbm, accepted_hbm,
    out_ref, part_ref, consts_ref,
    x_ref, gain_ref, wq_ref, wk_ref, wv_ref, wf_ref, qgain_ref, kgain_ref, hgain_ref, bias_ref, lengths_ref, accepted_ref, sems,
):
    kv = lax.axis_index("kv")
    tp = lax.axis_index("tp")
    column = pl.multiple_of(lax.div(kv, 2) * LANES, LANES)
    pairs = (
        (x_hbm, x_ref),
        (gain_hbm, gain_ref),
        (wq_hbm, wq_ref),
        (wk_hbm, wk_ref),
        (wv_hbm, wv_ref),
        (wf_hbm.at[:, pl.ds(column, LANES)], wf_ref),
        (qgain_hbm, qgain_ref),
        (kgain_hbm, kgain_ref),
        (hgain_hbm, hgain_ref),
        (bias_hbm, bias_ref),
        (lengths_hbm, lengths_ref),
        (accepted_hbm, accepted_ref),
    )
    copies = [pltpu.make_async_copy(a, b, sems.at[n]) for n, (a, b) in enumerate(pairs)]
    for copy in copies:
        copy.start()
    for copy in copies:
        copy.wait()
    at = tp * HEADS + lax.rem(kv, HEADS)
    spot = iota((1, 2 * HEADS), 1)
    bias = jnp.sum(jnp.where(spot == at, bias_ref[...], 0.0), axis=1, keepdims=True)
    consts_ref[0:1] = doubled(qgain_ref)
    consts_ref[1:2] = doubled(kgain_ref)
    consts_ref[2:3] = doubled(hgain_ref)
    consts_ref[3:4] = jnp.broadcast_to(bias, (1, LANES))
    consts_ref[4:5, 0:SEQS] = (lengths_ref[...] + accepted_ref[...]).astype(F32)
    x = x_ref[...].reshape(ROWS, DH).astype(F32)
    scaled = (x * gain_ref[...]).astype(BF16)
    blocks = [dot_nn(scaled, w[...]) for w in (wq_ref, wk_ref, wv_ref)]
    wide = jnp.concatenate([scaled, scaled], axis=1)
    half = (iota((ROWS, LANES), 1) // DH == lax.rem(kv, 2)).astype(F32).astype(BF16)
    gates = dot_nt(wf_ref[...], wide * half)
    own = jnp.where(tp == 0, gates[:HEADS], gates[HEADS:])
    squares = jnp.sum(x * x, axis=1, keepdims=True)
    diagonal = iota((ROWS, LANES), 0) == iota((ROWS, LANES), 1)
    square_row = jnp.sum(jnp.where(diagonal, squares, 0.0), axis=0, keepdims=True)[:, :DH]
    for s in range(SEQS):
        for c in range(QUARTERS):
            query, key, value = (
                packed(
                    *(
                        block[at : at + SUB, LANES * c : LANES * c + LANES]
                        for at in (PROPS * s, PROPS * s + SUB)
                    )
                )
                for block in blocks
            )
            for j in range(2):
                head = 2 * c + j
                peer = s * HEADS + head
                out_ref[SEND_A * peer : SEND_A * peer + SUB, :] = query[j]
                out_ref[SEND_A * peer + SUB : SEND_A * (peer + 1), :] = jnp.concatenate(
                    [own[head : head + 1], square_row], axis=1
                )
                highs = [x.astype(BF16).astype(F32) for x in (key[j], value[j])]
                part_ref[peer] = jnp.concatenate(
                    [highs[0], key[j] - highs[0], highs[1], value[j] - highs[1]], axis=0
                ).astype(BF16)


def head_scale(block):
    left = iota(block.shape, 1) < DH
    square = block * block
    first = jnp.sum(jnp.where(left, square, 0.0), axis=1, keepdims=True)
    second = jnp.sum(jnp.where(left, 0.0, square), axis=1, keepdims=True)
    return lax.rsqrt(jnp.where(left, first, second) / DH + EPSILON)


def finish_kernel(got_ref, part_ref, consts_ref, out_ref, row_ref, inverse_ref):
    s = lax.div(lax.axis_index("kv"), HEADS)
    query = got_ref[0:SUB]
    tail = got_ref[SUB:SEND_A]
    for p in range(1, N_KV):
        query = query + got_ref[SEND_A * p : SEND_A * p + SUB]
        tail = tail + got_ref[SEND_A * p + SUB : SEND_A * (p + 1)]
    other = swapped(jnp.broadcast_to(tail, (SUB, LANES)))[0:1]
    left = left_of((1, LANES))
    square = jnp.where(left, other, tail)
    gate_sum = jnp.where(left, tail, other)
    inverse_row = lax.rsqrt(square / (N_KV * DH) + EPSILON)
    lane = iota((SUB, LANES), 1)
    first = iota((SUB, LANES), 0) + s * PROPS
    upper = jnp.sum(jnp.where(lane == first, inverse_row, 0.0), axis=1, keepdims=True)
    lower = jnp.sum(jnp.where(lane == first + SUB, inverse_row, 0.0), axis=1, keepdims=True)
    inverse = jnp.where(left_of((SUB, LANES)), upper, lower)
    inverse_ref[...] = inverse
    query = query * inverse
    query = query * head_scale(query) * consts_ref[0:1]
    logit = gate_sum * inverse_row + consts_ref[3:4]
    small = jnp.exp(-jnp.abs(logit))
    one_more = 1.0 + small
    grown = jnp.where(
        one_more == 1.0, small, jnp.log(one_more) * small / jnp.where(one_more == 1.0, 1.0, one_more - 1.0)
    )
    row_ref[...] = jnp.minimum(logit, 0.0) - grown
    whole = query.astype(BF16)
    for p in range(N_KV):
        out_ref[p, 0:SUB] = whole
        out_ref[p, SUB:SEND_B] = part_ref[p]


def stage_kernel(
    key_hbm, value_hbm, gate_hbm, parents_ref, row_ref,
    key_ref, held_ref, gate_ref, bias_ref, new_key_hbm, new_value_hbm,
    rest_ref, sems,
):
    gate_load = pltpu.make_async_copy(gate_hbm, gate_ref, sems.at[2, 0])
    gate_load.start()
    targets = [key_ref.at[s] for s in range(SEQS)]
    targets += [held_ref.at[s] if s < HELD else rest_ref.at[s - HELD] for s in range(SEQS)]
    sources = [key_hbm.at[s] for s in range(SEQS)] + [value_hbm.at[s] for s in range(SEQS)]
    news = [new_key_hbm.at[s] for s in range(SEQS)] + [new_value_hbm.at[s] for s in range(SEQS)]
    loads = [pltpu.make_async_copy(a, b, sems.at[0, n]) for n, (a, b) in enumerate(zip(sources, targets))]
    stores = [pltpu.make_async_copy(a, b, sems.at[1, n]) for n, (a, b) in enumerate(zip(targets, news))]
    for load in loads:
        load.start()
    bias_ref[...] = tree_bias(parents_ref, row_ref)
    for load, store in zip(loads, stores):
        load.wait()
        store.start()
    gate_load.wait()
    for store in stores:
        store.wait()


def tree_bias(parents_ref, row_ref):
    s = lax.div(lax.axis_index("kv"), HEADS)
    square = (PROPS, PROPS)
    step = (iota(square, 0) == parents_ref[pl.ds(s, 1), :]).astype(F32)
    identity = (iota(square, 0) == iota(square, 1)).astype(F32)
    above = identity + step
    reach = step
    for _ in range(3):
        reach = dot_nn(reach, reach)
        above = above + dot_nn(above, reach)
    wide = (PROPS, LANES)
    wanted = iota(wide, 1) == iota(wide, 0) + s * PROPS
    gate = jnp.sum(jnp.where(wanted, row_ref[...], 0.0), axis=1, keepdims=True)
    path = jnp.sum(above * gate, axis=0, keepdims=True)
    return jnp.where(dot_nt(identity, above) > 0.5, -path, MASKED)


def attend_kernel(
    consts_ref, inverse_ref, row_ref, bias_ref, got_ref, key_ref, held_ref, gate_ref, value_hbm,
    out_ref, tree_ref, own_ref, rest_ref, weights_ref, sems,
):
    loads = {
        s: pltpu.make_async_copy(value_hbm.at[s], rest_ref.at[s - HELD], sems.at[s])
        for s in range(HELD, SEQS)
    }

    @pl.loop(HELD, SEQS)
    def _(s):
        pltpu.make_async_copy(value_hbm.at[s], rest_ref.at[s - HELD], sems.at[s]).start()

    sums = []
    for s in range(SEQS):
        raw = score_sequence(s, got_ref, key_ref)
        sums.append(weigh_sequence(s, raw, consts_ref[4:5, s : s + 1], gate_ref, weights_ref))
    attend_tree(consts_ref, inverse_ref, bias_ref, got_ref, tree_ref, own_ref)
    tail = row_ref[...]
    for s in range(SEQS):
        if s in loads:
            loads[s].wait()
        values = held_ref[s] if s < HELD else rest_ref[s - HELD]
        send_sequence(s, dot_nn(weights_ref[s], values), *sums[s], tail, out_ref)


def score_sequence(s, got_ref, key_ref):
    query = unpacked_rows(lambda p: got_ref[p, 0:SUB], s)
    wide = (HEADS * PROPS, WIDTH)
    own_head = iota(wide, 0) // PROPS == iota(wide, 1) // DH
    mask = jnp.where(own_head, 0.125, 0.0).astype(BF16)
    spread = jnp.concatenate([query] * HEADS, axis=0) * mask
    return dot_nt(spread, key_ref[s])


def weigh_sequence(s, scores, base, gate_ref, weights_ref):
    kv = lax.axis_index("kv")
    gate = gate_ref[s]
    edge_hit = (iota((HEADS, BLOCK), 1) + (kv * BLOCK + 1)).astype(F32) == base
    edge = jnp.sum(jnp.where(edge_hit, gate, 0.0), axis=1, keepdims=True)
    gates = jnp.concatenate(
        [jnp.broadcast_to(gate[h : h + 1], (PROPS, BLOCK)) for h in range(HEADS)], axis=0
    )
    position = (iota((HEADS * PROPS, BLOCK), 1) + kv * BLOCK).astype(F32)
    live = position < base
    scores = jnp.where(live, scores - gates, MASKED)
    peak = jnp.max(scores, axis=1, keepdims=True)
    weights = jnp.where(live, jnp.exp(scores - peak), 0.0)
    total = jnp.sum(weights, axis=1, keepdims=True)
    weights_ref[s] = weights.astype(BF16)
    some = total > 0.0
    safe = jnp.where(some, total, 1.0)
    log_sum = jnp.where(some, peak + jnp.log(safe), MASKED)
    return 1.0 / safe, log_sum, edge


def send_sequence(s, weighted, scale, log_sum, edge, tail, out_ref):
    weighted = weighted * scale
    lane = iota((PROPS, WIDTH), 1) // DH
    joined = jnp.zeros((PROPS, WIDTH), F32)
    for h in range(HEADS):
        joined = jnp.where(lane == h, weighted[h * PROPS : (h + 1) * PROPS], joined)
    whole = (LANES, LANES)
    spread = jnp.where(iota(whole, 0) == iota(whole, 1), log_sum, 0.0)
    log_row = jnp.sum(spread, axis=0, keepdims=True)
    lane = iota((1, LANES), 1)
    for c in range(QUARTERS):
        part = joined[:, LANES * c : LANES * c + LANES]
        both = packed(part[:SUB], part[SUB:])
        for j in range(2):
            h = 2 * c + j
            at = (s * HEADS + h) * SEND_C
            row = jnp.where(lane // PROPS == h, log_row, edge[h : h + 1])
            row = jnp.where(lane // DH == h // QUARTERS, row, tail)
            out_ref[at : at + SUB, :] = both[j]
            out_ref[at + SUB : at + SEND_C, :] = row


def attend_tree(consts_ref, inverse_ref, bias_ref, got_ref, tree_ref, own_ref):
    key = jnp.zeros((SUB, LANES), F32)
    value = jnp.zeros((SUB, LANES), F32)
    for p in range(N_KV):
        part = [got_ref[p, SUB * i : SUB * i + SUB].astype(F32) for i in range(1, 5)]
        key = key + (part[0] + part[1])
        value = value + (part[2] + part[3])
    inverse = inverse_ref[...]
    key = key * inverse
    key = (key * head_scale(key) * consts_ref[1:2]).astype(BF16).astype(F32)
    value = (value * inverse).astype(BF16).astype(F32)
    own_ref[...] = jnp.concatenate([key, value], axis=0).astype(BF16)
    query = got_ref[lax.axis_index("kv"), 0:SUB].astype(F32)
    left = left_of((PROPS, LANES))
    query, keys, values = (jnp.concatenate([x, swapped(x)], axis=0) for x in (query, key, value))
    query = jnp.where(left, query, 0.0).astype(BF16)
    bias = bias_ref[...]
    scores = dot_nt(query, keys.astype(BF16)) * 0.125 + bias
    peak = jnp.max(scores, axis=1, keepdims=True)
    weights = jnp.where(bias > 0.5 * MASKED, jnp.exp(scores - peak), 0.0)
    total = jnp.sum(weights, axis=1, keepdims=True)
    weighted = dot_nn(weights.astype(BF16), values.astype(BF16)) / total
    log_sum = peak + jnp.log(total)
    tree_ref[0:SUB] = jnp.where(left[:SUB], weighted[:SUB], swapped(weighted[SUB:]))
    tree_ref[SUB:] = jnp.where(left[:SUB], log_sum[:SUB], log_sum[SUB:])


def merge_kernel(got_ref, tree_ref, own_ref, consts_ref, out_ref):
    h = lax.rem(lax.axis_index("kv"), HEADS)
    shape = (LANES, LANES)
    source = iota(shape, 0)
    same = lax.rem(source, PROPS) // SUB == iota(shape, 1) // DH
    choose = jnp.where((source // PROPS == h) & same, 1.0, 0.0).astype(BF16)
    tile = (SUB, LANES)
    wanted = (iota(tile, 1) // PROPS == h) & (lax.rem(iota(tile, 1), SUB) == iota(tile, 0))
    edge_lane = lax.div(h, QUARTERS) * DH + lax.rem(h + 1, QUARTERS) * PROPS
    rows = [got_ref[SEND_C * p + SUB : SEND_C * (p + 1), :] for p in range(N_KV)]
    edge = rows[0]
    for row in rows[1:]:
        edge = edge + row
    edge = jnp.sum(jnp.where(iota((1, LANES), 1) == edge_lane, edge, 0.0), axis=1, keepdims=True)
    spread = jnp.concatenate([jnp.where(wanted, row, 0.0) for row in rows], axis=0)
    log_sums = jnp.zeros((N_KV * SUB, LANES), F32)
    for piece in pieces(spread):
        log_sums = log_sums + dot_nn(piece.astype(BF16), choose)
    top = log_sums[0:SUB]
    for p in range(1, N_KV):
        top = jnp.maximum(top, log_sums[SUB * p : SUB * p + SUB])
    tree_sum = tree_ref[SUB:] - edge
    top = jnp.maximum(top, tree_sum)
    weight = jnp.exp(tree_sum - top)
    below = weight
    above = weight * tree_ref[0:SUB]
    for p in range(N_KV):
        weight = jnp.exp(log_sums[SUB * p : SUB * p + SUB] - top)
        below = below + weight
        part = got_ref[SEND_C * p : SEND_C * p + SUB, :]
        above = above + weight * part
    attended = above / below
    normed = attended * head_scale(attended) * consts_ref[2:3]
    whole = normed.astype(BF16)
    own = own_ref[...]
    for p in range(N_KV):
        out_ref[p, 0:SUB] = whole
        out_ref[p, SUB:SEND_D] = own


def out_kernel(got_ref, w_ref, out_ref):
    rows = jnp.concatenate([unpacked_rows(lambda p: got_ref[p, 0:SUB], s) for s in range(SEQS)], axis=0)
    result = dot_nt(rows, w_ref[...])
    out_ref[...] = result.astype(BF16)


def write_kernel(
    consts_ref, parts_ref, got_ref, key_hbm, value_hbm, _k, _v,
    new_key_hbm, new_value_hbm, gates_ref, old_ref, rows_ref, sems,
):
    kv = lax.axis_index("kv")
    window = 2 * PROPS
    bases = [jnp.max(consts_ref[4:5, s : s + 1]).astype(jnp.int32) for s in range(SEQS)]
    firsts = [base - kv * BLOCK for base in bases]
    mine = [(first > -PROPS) & (first < BLOCK) for first in firsts]
    starts = [
        pl.multiple_of(jnp.minimum(lax.div(jnp.maximum(first, 0), PROPS) * PROPS, BLOCK - window), PROPS)
        for first in firsts
    ]

    def load(s, i):
        source = (key_hbm, value_hbm)[i].at[s, pl.ds(starts[s], window), :]
        return pltpu.make_async_copy(source, old_ref.at[2 * s + i], sems.at[0, 2 * s + i])

    def store(s, i):
        target = (new_key_hbm, new_value_hbm)[i].at[s, pl.ds(starts[s], window), :]
        return pltpu.make_async_copy(rows_ref.at[2 * s + i], target, sems.at[1, 2 * s + i])

    for s in range(SEQS):

        @pl.when(mine[s])
        def _():
            for i in range(2):
                load(s, i).start()

    for h in range(HEADS):
        row = parts_ref[SEND_C * h + SUB : SEND_C * (h + 1), :]
        row = jnp.where(lax.rem(kv, HEADS) < QUARTERS, row[:, DH:], row[:, :DH])
        for t in range(SEQS):
            at = PROPS * t
            gates_ref[t, h : h + 1, :] = row[:, at : at + PROPS]
    for s in range(SEQS):

        @pl.when(mine[s])
        def _():
            offset = starts[s] - firsts[s]
            placing = (iota((window, PROPS), 0) + offset == iota((window, PROPS), 1)).astype(F32).astype(BF16)
            line = iota((window, WIDTH), 0) + offset
            hit = (line >= 0) & (line < PROPS)
            for i in range(2):
                at = SUB * (i + 1)
                rows = unpacked_rows(lambda p: got_ref[p, at : at + SUB], s)
                written = dot_nn(placing, rows)
                load(s, i).wait()
                old = old_ref[2 * s + i].astype(F32)
                rows_ref[2 * s + i] = jnp.where(hit, written, old).astype(BF16)
                store(s, i).start()

    for s in range(SEQS):

        @pl.when(mine[s])
        def _():
            for i in range(2):
                store(s, i).wait()


def exchange(array):
    return lax.all_to_all(array, "kv", split_axis=0, concat_axis=0, tiled=True)


def shards(
    tokens,
    norm_gain,
    w_query,
    w_key,
    w_value,
    w_forget,
    forget_bias,
    query_gain,
    key_gain,
    head_gain,
    w_out,
    key_cache,
    value_cache,
    gate_cache,
    lengths,
    accepted,
    parents,
):
    def line(gain):
        return gain.reshape(1, DH)

    def limit(size):
        return pltpu.CompilerParams(vmem_limit_bytes=size * 2**20)

    cache = jax.ShapeDtypeStruct(key_cache.shape, BF16)
    sent, part, consts = pl.pallas_call(
        project_kernel,
        out_shape=(
            jax.ShapeDtypeStruct((N_KV * SEND_A, LANES), F32),
            jax.ShapeDtypeStruct((N_KV, SEND_KV, LANES), BF16),
            jax.ShapeDtypeStruct((SUB, LANES), F32),
        ),
        in_specs=[hbm()] * 12,
        out_specs=(vmem(), vmem(), vmem()),
        scratch_shapes=[
            pltpu.VMEM((SEQS, PROPS, DH), BF16),
            pltpu.VMEM((1, DH), F32),
            pltpu.VMEM((DH, WIDTH), BF16),
            pltpu.VMEM((DH, WIDTH), BF16),
            pltpu.VMEM((DH, WIDTH), BF16),
            pltpu.VMEM((2 * HEADS, LANES), BF16),
            pltpu.VMEM((1, DH), F32),
            pltpu.VMEM((1, DH), F32),
            pltpu.VMEM((1, DH), F32),
            pltpu.VMEM((1, 2 * HEADS), F32),
            pltpu.VMEM((1, SEQS), jnp.int32),
            pltpu.VMEM((1, SEQS), jnp.int32),
            pltpu.SemaphoreType.DMA((12,)),
        ],
        cost_estimate=cost(13_000_000, 700_000),
        compiler_params=limit(8),
        name="project",
    )(
        *map(
            stay,
            (
                tokens, line(norm_gain), w_query, w_key, w_value, w_forget.T,
                line(query_gain), line(key_gain), line(head_gain), forget_bias.reshape(1, 2 * HEADS),
                lengths.reshape(1, SEQS), accepted.reshape(1, SEQS),
            ),
        )
    )
    got = exchange(sent.reshape(N_KV, 1, SEND_A * LANES)).reshape(N_KV * SEND_A, LANES)
    sent, gate_row, inverse = pl.pallas_call(
        finish_kernel,
        out_shape=(
            jax.ShapeDtypeStruct((N_KV, SEND_B, LANES), BF16),
            jax.ShapeDtypeStruct((1, LANES), F32),
            jax.ShapeDtypeStruct((SUB, LANES), F32),
        ),
        in_specs=[vmem()] * 3,
        out_specs=(vmem(), vmem(), vmem()),
        cost_estimate=cost(1_000_000, 700_000),
        compiler_params=limit(8),
        name="finish",
    )(got, part, consts)
    rows = exchange(sent)
    gate_row, key_cache, value_cache, gate_cache = lax.optimization_barrier(
        (gate_row, key_cache, value_cache, gate_cache)
    )
    keys, held, gate_block, bias, new_keys, new_values = pl.pallas_call(
        stage_kernel,
        out_shape=(
            cache,
            jax.ShapeDtypeStruct((HELD, BLOCK, WIDTH), BF16),
            jax.ShapeDtypeStruct(gate_cache.shape, F32),
            jax.ShapeDtypeStruct((PROPS, PROPS), F32),
            pltpu.HBM(key_cache.shape, BF16),
            pltpu.HBM(value_cache.shape, BF16),
        ),
        in_specs=[hbm()] * 3 + [vmem()] * 2,
        out_specs=(vmem(),) * 4 + (hbm(), hbm()),
        scratch_shapes=[
            pltpu.VMEM((SEQS - HELD, BLOCK, WIDTH), BF16),
            pltpu.SemaphoreType.DMA((3, 2 * SEQS)),
        ],
        cost_estimate=cost(500_000_000, 8_500_000),
        compiler_params=limit(8),
        name="stage",
    )(stay(key_cache), stay(value_cache), stay(gate_cache), parents, gate_row)
    rows, keys, held, gate_block = lax.optimization_barrier((rows, keys, held, gate_block))
    sent, tree, own = pl.pallas_call(
        attend_kernel,
        out_shape=(
            jax.ShapeDtypeStruct((N_KV * SEND_C, LANES), F32),
            jax.ShapeDtypeStruct((2 * SUB, LANES), F32),
            jax.ShapeDtypeStruct((2 * SUB, LANES), BF16),
        ),
        in_specs=[vmem()] * 8 + [hbm()],
        out_specs=(vmem(), vmem(), vmem()),
        scratch_shapes=[
            pltpu.VMEM((SEQS - HELD, BLOCK, WIDTH), BF16),
            pltpu.VMEM((SEQS, HEADS * PROPS, BLOCK), BF16),
            pltpu.SemaphoreType.DMA((SEQS + 1,)),
        ],
        cost_estimate=cost(600_000_000, 4_500_000),
        compiler_params=limit(16),
        name="attend",
    )(consts, inverse, gate_row, bias, rows, keys, held, gate_block, stay(value_cache))
    parts = exchange(sent.reshape(N_KV, 1, SEND_C * LANES)).reshape(N_KV * SEND_C, LANES)
    sent = pl.pallas_call(
        merge_kernel,
        out_shape=jax.ShapeDtypeStruct((N_KV, SEND_D, LANES), BF16),
        in_specs=[vmem()] * 4,
        out_specs=vmem(),
        cost_estimate=cost(8_000_000, 200_000),
        compiler_params=limit(8),
        name="merge",
    )(parts, tree, own, consts)
    normed = exchange(sent)
    term = pl.pallas_call(
        out_kernel,
        out_shape=jax.ShapeDtypeStruct((ROWS, DH), BF16),
        in_specs=[vmem()] * 2,
        out_specs=vmem(),
        cost_estimate=cost(4_000_000, 150_000),
        compiler_params=limit(8),
        name="out",
    )(normed, w_out.T)
    other = lax.ppermute(term, "tp", [(0, 1), (1, 0)])
    term, parts = lax.optimization_barrier((term, parts))
    new_keys, new_values, gates = pl.pallas_call(
        write_kernel,
        out_shape=(cache, cache, jax.ShapeDtypeStruct((SEQS, HEADS, PROPS), F32)),
        in_specs=[vmem()] * 3 + [hbm()] * 4,
        out_specs=(hbm(), hbm(), vmem()),
        scratch_shapes=[
            pltpu.VMEM((2 * SEQS, 2 * PROPS, WIDTH), BF16),
            pltpu.VMEM((2 * SEQS, 2 * PROPS, WIDTH), BF16),
            pltpu.SemaphoreType.DMA((2, 2 * SEQS)),
        ],
        input_output_aliases={5: 0, 6: 1},
        cost_estimate=cost(60_000_000, 1_000_000),
        compiler_params=limit(8),
        name="write",
    )(
        consts, parts, normed, stay(key_cache), stay(value_cache), stay(new_keys), stay(new_values)
    )
    layer_out = (term.astype(F32) + other.astype(F32)).astype(BF16)
    return (layer_out.reshape(SEQS, PROPS, DH), new_keys, new_values, gates.transpose(0, 2, 1))


def solution(mesh):
    placed = (
        P("dp", None, "kv"),
        P("kv"),
        P("kv", "tp"),
        P("kv", "tp"),
        P("kv", "tp"),
        P(),
        P(),
        P(),
        P(),
        P(),
        P("tp", "kv"),
        P("dp", "kv", "tp"),
        P("dp", "kv", "tp"),
        P("dp", "tp", "kv"),
        P("dp"),
        P("dp"),
        P("dp", None),
    )
    return jax.shard_map(
        shards,
        mesh=mesh,
        in_specs=placed,
        out_specs=(
            P("dp", None, "kv"),
            P("dp", "kv", "tp"),
            P("dp", "kv", "tp"),
            P("dp", None, "tp"),
        ),
        check_vma=False,
    )
```

```python
import jax
import jax.numpy as jnp
from jax import lax
from jax.experimental import pallas as pl
from jax.experimental.pallas import tpu as pltpu
from jax.sharding import PartitionSpec as P

EPSILON = 1e-06
MASKED = -1e30
F32 = jnp.float32
BF16 = jnp.bfloat16

LANES = 128
SUB = 8
N_KV = 32
QUARTERS = 4
ROWS = 64
HEADS = 8
DH = 64
WIDTH = 512
PROPS = 16
SEQS = 4
BLOCK = 512
SEND_A = 9
SEND_KV = 24
SEND_B = SUB + SEND_KV
SEND_C = 9
SEND_D = 24
HELD = 2


def iota(shape, dim):
    return lax.broadcasted_iota(jnp.int32, shape, dim)


def dot_nn(a, b):
    return lax.dot_general(a, b, (((1,), (0,)), ((), ())), preferred_element_type=F32)


def dot_nt(a, b):
    return lax.dot_general(a, b, (((1,), (1,)), ((), ())), preferred_element_type=F32)


def pieces(x):
    high = x.astype(BF16).astype(F32)
    rest = x - high
    middle = rest.astype(BF16).astype(F32)
    return high, middle, rest - middle


def left_of(shape):
    return iota(shape, len(shape) - 1) < DH


def swapped(block):
    return pltpu.roll(block, DH, 1)


def packed(top, bottom):
    left = left_of(top.shape)
    return jnp.where(left, top, swapped(bottom)), jnp.where(left, swapped(top), bottom)


def unpacked_rows(read, s):
    tiles = []
    for c in range(QUARTERS):
        even, odd = (read(s * HEADS + 2 * c + j).astype(F32) for j in range(2))
        tiles.append(jnp.concatenate(packed(even, odd), axis=0))
    return jnp.concatenate(tiles, axis=1).astype(BF16)


def vmem():
    return pl.BlockSpec(memory_space=pltpu.VMEM)


def stay(array):
    return pltpu.with_memory_space_constraint(array, pltpu.HBM)


def hbm():
    return pl.BlockSpec(memory_space=pltpu.HBM)


def cost(flops, moved):
    return pl.CostEstimate(flops=flops, bytes_accessed=moved, transcendentals=0)


def doubled(gain_ref):
    gain = gain_ref[...]
    return jnp.concatenate([gain, gain], axis=1)


def project_kernel(
    x_hbm, gain_hbm, wq_hbm, wk_hbm, wv_hbm, wf_hbm, qgain_hbm, kgain_hbm, hgain_hbm, bias_hbm, lengths_hbm, accepted_hbm,
    out_ref, part_ref, consts_ref,
    x_ref, gain_ref, wq_ref, wk_ref, wv_ref, wf_ref, qgain_ref, kgain_ref, hgain_ref, bias_ref, lengths_ref, accepted_ref, sems,
):
    kv = lax.axis_index("kv")
    tp = lax.axis_index("tp")
    column = pl.multiple_of(lax.div(kv, 2) * LANES, LANES)
    pairs = (
        (x_hbm, x_ref),
        (gain_hbm, gain_ref),
        (wq_hbm, wq_ref),
        (wk_hbm, wk_ref),
        (wv_hbm, wv_ref),
        (wf_hbm.at[:, pl.ds(column, LANES)], wf_ref),
        (qgain_hbm, qgain_ref),
        (kgain_hbm, kgain_ref),
        (hgain_hbm, hgain_ref),
        (bias_hbm, bias_ref),
        (lengths_hbm, lengths_ref),
        (accepted_hbm, accepted_ref),
    )
    copies = [pltpu.make_async_copy(a, b, sems.at[n]) for n, (a, b) in enumerate(pairs)]
    for copy in copies:
        copy.start()
    for copy in copies:
        copy.wait()
    at = tp * HEADS + lax.rem(kv, HEADS)
    spot = iota((1, 2 * HEADS), 1)
    bias = jnp.sum(jnp.where(spot == at, bias_ref[...], 0.0), axis=1, keepdims=True)
    consts_ref[0:1] = doubled(qgain_ref)
    consts_ref[1:2] = doubled(kgain_ref)
    consts_ref[2:3] = doubled(hgain_ref)
    consts_ref[3:4] = jnp.broadcast_to(bias, (1, LANES))
    consts_ref[4:5, 0:SEQS] = (lengths_ref[...] + accepted_ref[...]).astype(F32)
    x = x_ref[...].reshape(ROWS, DH).astype(F32)
    scaled = (x * gain_ref[...]).astype(BF16)
    blocks = [dot_nn(scaled, w[...]) for w in (wq_ref, wk_ref, wv_ref)]
    wide = jnp.concatenate([scaled, scaled], axis=1)
    half = (iota((ROWS, LANES), 1) // DH == lax.rem(kv, 2)).astype(F32).astype(BF16)
    gates = dot_nt(wf_ref[...], wide * half)
    own = jnp.where(tp == 0, gates[:HEADS], gates[HEADS:])
    squares = jnp.sum(x * x, axis=1, keepdims=True)
    diagonal = iota((ROWS, LANES), 0) == iota((ROWS, LANES), 1)
    square_row = jnp.sum(jnp.where(diagonal, squares, 0.0), axis=0, keepdims=True)[:, :DH]
    for s in range(SEQS):
        for c in range(QUARTERS):
            query, key, value = (
                packed(
                    *(
                        block[at : at + SUB, LANES * c : LANES * c + LANES]
                        for at in (PROPS * s, PROPS * s + SUB)
                    )
                )
                for block in blocks
            )
            for j in range(2):
                head = 2 * c + j
                peer = s * HEADS + head
                out_ref[SEND_A * peer : SEND_A * peer + SUB, :] = query[j]
                out_ref[SEND_A * peer + SUB : SEND_A * (peer + 1), :] = jnp.concatenate(
                    [own[head : head + 1], square_row], axis=1
                )
                high = key[j].astype(BF16).astype(F32)
                part_ref[peer] = jnp.concatenate([high, key[j] - high, value[j]], axis=0).astype(BF16)


def head_scale(block):
    left = iota(block.shape, 1) < DH
    square = block * block
    first = jnp.sum(jnp.where(left, square, 0.0), axis=1, keepdims=True)
    second = jnp.sum(jnp.where(left, 0.0, square), axis=1, keepdims=True)
    return lax.rsqrt(jnp.where(left, first, second) / DH + EPSILON)


def finish_kernel(got_ref, part_ref, consts_ref, out_ref, row_ref, inverse_ref):
    s = lax.div(lax.axis_index("kv"), HEADS)
    query = got_ref[0:SUB]
    tail = got_ref[SUB:SEND_A]
    for p in range(1, N_KV):
        query = query + got_ref[SEND_A * p : SEND_A * p + SUB]
        tail = tail + got_ref[SEND_A * p + SUB : SEND_A * (p + 1)]
    other = swapped(jnp.broadcast_to(tail, (SUB, LANES)))[0:1]
    left = left_of((1, LANES))
    square = jnp.where(left, other, tail)
    gate_sum = jnp.where(left, tail, other)
    inverse_row = lax.rsqrt(square / (N_KV * DH) + EPSILON)
    lane = iota((SUB, LANES), 1)
    first = iota((SUB, LANES), 0) + s * PROPS
    upper = jnp.sum(jnp.where(lane == first, inverse_row, 0.0), axis=1, keepdims=True)
    lower = jnp.sum(jnp.where(lane == first + SUB, inverse_row, 0.0), axis=1, keepdims=True)
    inverse = jnp.where(left_of((SUB, LANES)), upper, lower)
    inverse_ref[...] = inverse
    query = query * inverse
    query = query * head_scale(query) * consts_ref[0:1]
    logit = gate_sum * inverse_row + consts_ref[3:4]
    small = jnp.exp(-jnp.abs(logit))
    one_more = 1.0 + small
    grown = jnp.where(
        one_more == 1.0, small, jnp.log(one_more) * small / jnp.where(one_more == 1.0, 1.0, one_more - 1.0)
    )
    row_ref[...] = jnp.minimum(logit, 0.0) - grown
    whole = query.astype(BF16)
    for p in range(N_KV):
        out_ref[p, 0:SUB] = whole
        out_ref[p, SUB:SEND_B] = part_ref[p]


def stage_kernel(
    key_hbm, value_hbm, gate_hbm, parents_ref, row_ref,
    key_ref, held_ref, gate_ref, bias_ref, new_key_hbm, new_value_hbm,
    rest_ref, sems,
):
    gate_load = pltpu.make_async_copy(gate_hbm, gate_ref, sems.at[2, 0])
    gate_load.start()
    targets = [key_ref.at[s] for s in range(SEQS)]
    targets += [held_ref.at[s] if s < HELD else rest_ref.at[s - HELD] for s in range(SEQS)]
    sources = [key_hbm.at[s] for s in range(SEQS)] + [value_hbm.at[s] for s in range(SEQS)]
    news = [new_key_hbm.at[s] for s in range(SEQS)] + [new_value_hbm.at[s] for s in range(SEQS)]
    loads = [pltpu.make_async_copy(a, b, sems.at[0, n]) for n, (a, b) in enumerate(zip(sources, targets))]
    stores = [pltpu.make_async_copy(a, b, sems.at[1, n]) for n, (a, b) in enumerate(zip(targets, news))]
    for load in loads:
        load.start()
    bias_ref[...] = tree_bias(parents_ref, row_ref)
    for load, store in zip(loads, stores):
        load.wait()
        store.start()
    gate_load.wait()
    for store in stores:
        store.wait()


def tree_bias(parents_ref, row_ref):
    s = lax.div(lax.axis_index("kv"), HEADS)
    square = (PROPS, PROPS)
    step = (iota(square, 0) == parents_ref[pl.ds(s, 1), :]).astype(F32)
    identity = (iota(square, 0) == iota(square, 1)).astype(F32)
    above = identity + step
    reach = step
    for _ in range(3):
        reach = dot_nn(reach, reach)
        above = above + dot_nn(above, reach)
    wide = (PROPS, LANES)
    wanted = iota(wide, 1) == iota(wide, 0) + s * PROPS
    gate = jnp.sum(jnp.where(wanted, row_ref[...], 0.0), axis=1, keepdims=True)
    path = jnp.sum(above * gate, axis=0, keepdims=True)
    return jnp.where(dot_nt(identity, above) > 0.5, -path, MASKED)


def attend_kernel(
    consts_ref, inverse_ref, row_ref, bias_ref, got_ref, key_ref, held_ref, gate_ref, value_hbm,
    out_ref, tree_ref, own_ref, rest_ref, weights_ref, sems,
):
    loads = {
        s: pltpu.make_async_copy(value_hbm.at[s], rest_ref.at[s - HELD], sems.at[s])
        for s in range(HELD, SEQS)
    }

    @pl.loop(HELD, SEQS)
    def _(s):
        pltpu.make_async_copy(value_hbm.at[s], rest_ref.at[s - HELD], sems.at[s]).start()

    sums = []
    for s in range(SEQS):
        raw = score_sequence(s, got_ref, key_ref)
        sums.append(weigh_sequence(s, raw, consts_ref[4:5, s : s + 1], gate_ref, weights_ref))
    attend_tree(consts_ref, inverse_ref, bias_ref, got_ref, tree_ref, own_ref)
    tail = row_ref[...]
    for s in range(SEQS):
        if s == HELD:
            for load in loads.values():
                load.wait()
        values = held_ref[s] if s < HELD else rest_ref[s - HELD]
        send_sequence(s, dot_nn(weights_ref[s], values), *sums[s], tail, out_ref)


def score_sequence(s, got_ref, key_ref):
    query = unpacked_rows(lambda p: got_ref[p, 0:SUB], s)
    wide = (HEADS * PROPS, WIDTH)
    own_head = iota(wide, 0) // PROPS == iota(wide, 1) // DH
    mask = jnp.where(own_head, 0.125, 0.0).astype(BF16)
    spread = jnp.concatenate([query] * HEADS, axis=0) * mask
    return dot_nt(spread, key_ref[s])


def weigh_sequence(s, scores, base, gate_ref, weights_ref):
    kv = lax.axis_index("kv")
    gate = gate_ref[s]
    edge_hit = (iota((HEADS, BLOCK), 1) + (kv * BLOCK + 1)).astype(F32) == base
    edge = jnp.sum(jnp.where(edge_hit, gate, 0.0), axis=1, keepdims=True)
    gates = jnp.concatenate(
        [jnp.broadcast_to(gate[h : h + 1], (PROPS, BLOCK)) for h in range(HEADS)], axis=0
    )
    position = (iota((HEADS * PROPS, BLOCK), 1) + kv * BLOCK).astype(F32)
    live = position < base
    scores = jnp.where(live, scores - gates, MASKED)
    peak = jnp.max(scores, axis=1, keepdims=True)
    weights = jnp.where(live, jnp.exp(scores - peak), 0.0)
    total = jnp.sum(weights, axis=1, keepdims=True)
    weights_ref[s] = weights.astype(BF16)
    some = total > 0.0
    safe = jnp.where(some, total, 1.0)
    log_sum = jnp.where(some, peak + jnp.log(safe), MASKED)
    return 1.0 / safe, log_sum, edge


def send_sequence(s, weighted, scale, log_sum, edge, tail, out_ref):
    weighted = weighted * scale
    lane = iota((PROPS, WIDTH), 1) // DH
    joined = jnp.zeros((PROPS, WIDTH), F32)
    for h in range(HEADS):
        joined = jnp.where(lane == h, weighted[h * PROPS : (h + 1) * PROPS], joined)
    whole = (LANES, LANES)
    spread = jnp.where(iota(whole, 0) == iota(whole, 1), log_sum, 0.0)
    log_row = jnp.sum(spread, axis=0, keepdims=True)
    lane = iota((1, LANES), 1)
    for c in range(QUARTERS):
        part = joined[:, LANES * c : LANES * c + LANES]
        both = packed(part[:SUB], part[SUB:])
        for j in range(2):
            h = 2 * c + j
            at = (s * HEADS + h) * SEND_C
            row = jnp.where(lane // PROPS == h, log_row, edge[h : h + 1])
            row = jnp.where(lane // DH == h // QUARTERS, row, tail)
            out_ref[at : at + SUB, :] = both[j]
            out_ref[at + SUB : at + SEND_C, :] = row


def attend_tree(consts_ref, inverse_ref, bias_ref, got_ref, tree_ref, own_ref):
    key = jnp.zeros((SUB, LANES), F32)
    value = jnp.zeros((SUB, LANES), F32)
    for p in range(N_KV):
        high, low, part = (got_ref[p, SUB * i : SUB * i + SUB].astype(F32) for i in range(1, 4))
        key = key + (high + low)
        value = value + part
    inverse = inverse_ref[...]
    key = key * inverse
    key = (key * head_scale(key) * consts_ref[1:2]).astype(BF16).astype(F32)
    value = (value * inverse).astype(BF16).astype(F32)
    own_ref[...] = jnp.concatenate([key, value], axis=0).astype(BF16)
    query = got_ref[lax.axis_index("kv"), 0:SUB].astype(F32)
    left = left_of((PROPS, LANES))
    query, keys, values = (jnp.concatenate([x, swapped(x)], axis=0) for x in (query, key, value))
    query = jnp.where(left, query, 0.0).astype(BF16)
    bias = bias_ref[...]
    scores = dot_nt(query, keys.astype(BF16)) * 0.125 + bias
    peak = jnp.max(scores, axis=1, keepdims=True)
    weights = jnp.where(bias > 0.5 * MASKED, jnp.exp(scores - peak), 0.0)
    total = jnp.sum(weights, axis=1, keepdims=True)
    weighted = dot_nn(weights.astype(BF16), values.astype(BF16)) / total
    log_sum = peak + jnp.log(total)
    tree_ref[0:SUB] = jnp.where(left[:SUB], weighted[:SUB], swapped(weighted[SUB:]))
    tree_ref[SUB:] = jnp.where(left[:SUB], log_sum[:SUB], log_sum[SUB:])


def merge_kernel(got_ref, tree_ref, own_ref, consts_ref, out_ref):
    h = lax.rem(lax.axis_index("kv"), HEADS)
    shape = (LANES, LANES)
    source = iota(shape, 0)
    same = lax.rem(source, PROPS) // SUB == iota(shape, 1) // DH
    choose = jnp.where((source // PROPS == h) & same, 1.0, 0.0).astype(BF16)
    tile = (SUB, LANES)
    wanted = (iota(tile, 1) // PROPS == h) & (lax.rem(iota(tile, 1), SUB) == iota(tile, 0))
    edge_lane = lax.div(h, QUARTERS) * DH + lax.rem(h + 1, QUARTERS) * PROPS
    rows = [got_ref[SEND_C * p + SUB : SEND_C * (p + 1), :] for p in range(N_KV)]
    edge = rows[0]
    for row in rows[1:]:
        edge = edge + row
    edge = jnp.sum(jnp.where(iota((1, LANES), 1) == edge_lane, edge, 0.0), axis=1, keepdims=True)
    spread = jnp.concatenate([jnp.where(wanted, row, 0.0) for row in rows], axis=0)
    log_sums = jnp.zeros((N_KV * SUB, LANES), F32)
    for piece in pieces(spread):
        log_sums = log_sums + dot_nn(piece.astype(BF16), choose)
    top = log_sums[0:SUB]
    for p in range(1, N_KV):
        top = jnp.maximum(top, log_sums[SUB * p : SUB * p + SUB])
    tree_sum = tree_ref[SUB:] - edge
    top = jnp.maximum(top, tree_sum)
    weight = jnp.exp(tree_sum - top)
    below = weight
    above = weight * tree_ref[0:SUB]
    for p in range(N_KV):
        weight = jnp.exp(log_sums[SUB * p : SUB * p + SUB] - top)
        below = below + weight
        part = got_ref[SEND_C * p : SEND_C * p + SUB, :]
        above = above + weight * part
    attended = above / below
    normed = attended * head_scale(attended) * consts_ref[2:3]
    whole = normed.astype(BF16)
    own = own_ref[...]
    for p in range(N_KV):
        out_ref[p, 0:SUB] = whole
        out_ref[p, SUB:SEND_D] = own


def out_kernel(got_ref, w_ref, out_ref):
    rows = jnp.concatenate([unpacked_rows(lambda p: got_ref[p, 0:SUB], s) for s in range(SEQS)], axis=0)
    result = dot_nt(rows, w_ref[...])
    out_ref[...] = result.astype(BF16)


def write_kernel(
    consts_ref, parts_ref, got_ref, key_hbm, value_hbm, _k, _v,
    new_key_hbm, new_value_hbm, gates_ref, old_ref, rows_ref, sems,
):
    kv = lax.axis_index("kv")
    window = 2 * PROPS
    bases = [jnp.max(consts_ref[4:5, s : s + 1]).astype(jnp.int32) for s in range(SEQS)]
    firsts = [base - kv * BLOCK for base in bases]
    mine = [(first > -PROPS) & (first < BLOCK) for first in firsts]
    starts = [
        pl.multiple_of(jnp.minimum(lax.div(jnp.maximum(first, 0), PROPS) * PROPS, BLOCK - window), PROPS)
        for first in firsts
    ]

    def load(s, i):
        source = (key_hbm, value_hbm)[i].at[s, pl.ds(starts[s], window), :]
        return pltpu.make_async_copy(source, old_ref.at[2 * s + i], sems.at[0, 2 * s + i])

    def store(s, i):
        target = (new_key_hbm, new_value_hbm)[i].at[s, pl.ds(starts[s], window), :]
        return pltpu.make_async_copy(rows_ref.at[2 * s + i], target, sems.at[1, 2 * s + i])

    for s in range(SEQS):

        @pl.when(mine[s])
        def _():
            for i in range(2):
                load(s, i).start()

    for h in range(HEADS):
        row = parts_ref[SEND_C * h + SUB : SEND_C * (h + 1), :]
        row = jnp.where(lax.rem(kv, HEADS) < QUARTERS, row[:, DH:], row[:, :DH])
        for t in range(SEQS):
            at = PROPS * t
            gates_ref[t, h : h + 1, :] = row[:, at : at + PROPS]
    for s in range(SEQS):

        @pl.when(mine[s])
        def _():
            offset = starts[s] - firsts[s]
            placing = (iota((window, PROPS), 0) + offset == iota((window, PROPS), 1)).astype(F32).astype(BF16)
            line = iota((window, WIDTH), 0) + offset
            hit = (line >= 0) & (line < PROPS)
            for i in range(2):
                at = SUB * (i + 1)
                rows = unpacked_rows(lambda p: got_ref[p, at : at + SUB], s)
                written = dot_nn(placing, rows)
                load(s, i).wait()
                old = old_ref[2 * s + i].astype(F32)
                rows_ref[2 * s + i] = jnp.where(hit, written, old).astype(BF16)
                store(s, i).start()

    for s in range(SEQS):

        @pl.when(mine[s])
        def _():
            for i in range(2):
                store(s, i).wait()


def exchange(array):
    return lax.all_to_all(array, "kv", split_axis=0, concat_axis=0, tiled=True)


def shards(
    tokens,
    norm_gain,
    w_query,
    w_key,
    w_value,
    w_forget,
    forget_bias,
    query_gain,
    key_gain,
    head_gain,
    w_out,
    key_cache,
    value_cache,
    gate_cache,
    lengths,
    accepted,
    parents,
):
    def line(gain):
        return gain.reshape(1, DH)

    def limit(size):
        return pltpu.CompilerParams(vmem_limit_bytes=size * 2**20)

    cache = jax.ShapeDtypeStruct(key_cache.shape, BF16)
    sent, part, consts = pl.pallas_call(
        project_kernel,
        out_shape=(
            jax.ShapeDtypeStruct((N_KV * SEND_A, LANES), F32),
            jax.ShapeDtypeStruct((N_KV, SEND_KV, LANES), BF16),
            jax.ShapeDtypeStruct((SUB, LANES), F32),
        ),
        in_specs=[hbm()] * 12,
        out_specs=(vmem(), vmem(), vmem()),
        scratch_shapes=[
            pltpu.VMEM((SEQS, PROPS, DH), BF16),
            pltpu.VMEM((1, DH), F32),
            pltpu.VMEM((DH, WIDTH), BF16),
            pltpu.VMEM((DH, WIDTH), BF16),
            pltpu.VMEM((DH, WIDTH), BF16),
            pltpu.VMEM((2 * HEADS, LANES), BF16),
            pltpu.VMEM((1, DH), F32),
            pltpu.VMEM((1, DH), F32),
            pltpu.VMEM((1, DH), F32),
            pltpu.VMEM((1, 2 * HEADS), F32),
            pltpu.VMEM((1, SEQS), jnp.int32),
            pltpu.VMEM((1, SEQS), jnp.int32),
            pltpu.SemaphoreType.DMA((12,)),
        ],
        cost_estimate=cost(13_000_000, 700_000),
        compiler_params=limit(8),
        name="project",
    )(
        *map(
            stay,
            (
                tokens, line(norm_gain), w_query, w_key, w_value, w_forget.T,
                line(query_gain), line(key_gain), line(head_gain), forget_bias.reshape(1, 2 * HEADS),
                lengths.reshape(1, SEQS), accepted.reshape(1, SEQS),
            ),
        )
    )
    got = exchange(sent.reshape(N_KV, 1, SEND_A * LANES)).reshape(N_KV * SEND_A, LANES)
    sent, gate_row, inverse = pl.pallas_call(
        finish_kernel,
        out_shape=(
            jax.ShapeDtypeStruct((N_KV, SEND_B, LANES), BF16),
            jax.ShapeDtypeStruct((1, LANES), F32),
            jax.ShapeDtypeStruct((SUB, LANES), F32),
        ),
        in_specs=[vmem()] * 3,
        out_specs=(vmem(), vmem(), vmem()),
        cost_estimate=cost(1_000_000, 700_000),
        compiler_params=limit(8),
        name="finish",
    )(got, part, consts)
    rows = exchange(sent)
    gate_row, key_cache, value_cache, gate_cache = lax.optimization_barrier(
        (gate_row, key_cache, value_cache, gate_cache)
    )
    keys, held, gate_block, bias, new_keys, new_values = pl.pallas_call(
        stage_kernel,
        out_shape=(
            cache,
            jax.ShapeDtypeStruct((HELD, BLOCK, WIDTH), BF16),
            jax.ShapeDtypeStruct(gate_cache.shape, F32),
            jax.ShapeDtypeStruct((PROPS, PROPS), F32),
            pltpu.HBM(key_cache.shape, BF16),
            pltpu.HBM(value_cache.shape, BF16),
        ),
        in_specs=[hbm()] * 3 + [vmem()] * 2,
        out_specs=(vmem(),) * 4 + (hbm(), hbm()),
        scratch_shapes=[
            pltpu.VMEM((SEQS - HELD, BLOCK, WIDTH), BF16),
            pltpu.SemaphoreType.DMA((3, 2 * SEQS)),
        ],
        cost_estimate=cost(500_000_000, 8_500_000),
        compiler_params=limit(8),
        name="stage",
    )(stay(key_cache), stay(value_cache), stay(gate_cache), parents, gate_row)
    rows, keys, held, gate_block = lax.optimization_barrier((rows, keys, held, gate_block))
    sent, tree, own = pl.pallas_call(
        attend_kernel,
        out_shape=(
            jax.ShapeDtypeStruct((N_KV * SEND_C, LANES), F32),
            jax.ShapeDtypeStruct((2 * SUB, LANES), F32),
            jax.ShapeDtypeStruct((2 * SUB, LANES), BF16),
        ),
        in_specs=[vmem()] * 8 + [hbm()],
        out_specs=(vmem(), vmem(), vmem()),
        scratch_shapes=[
            pltpu.VMEM((SEQS - HELD, BLOCK, WIDTH), BF16),
            pltpu.VMEM((SEQS, HEADS * PROPS, BLOCK), BF16),
            pltpu.SemaphoreType.DMA((SEQS + 1,)),
        ],
        cost_estimate=cost(600_000_000, 4_500_000),
        compiler_params=limit(16),
        name="attend",
    )(consts, inverse, gate_row, bias, rows, keys, held, gate_block, stay(value_cache))
    parts = exchange(sent.reshape(N_KV, 1, SEND_C * LANES)).reshape(N_KV * SEND_C, LANES)
    sent = pl.pallas_call(
        merge_kernel,
        out_shape=jax.ShapeDtypeStruct((N_KV, SEND_D, LANES), BF16),
        in_specs=[vmem()] * 4,
        out_specs=vmem(),
        cost_estimate=cost(8_000_000, 200_000),
        compiler_params=limit(8),
        name="merge",
    )(parts, tree, own, consts)
    normed = exchange(sent)
    term = pl.pallas_call(
        out_kernel,
        out_shape=jax.ShapeDtypeStruct((ROWS, DH), BF16),
        in_specs=[vmem()] * 2,
        out_specs=vmem(),
        cost_estimate=cost(4_000_000, 150_000),
        compiler_params=limit(8),
        name="out",
    )(normed, w_out.T)
    other = lax.ppermute(term, "tp", [(0, 1), (1, 0)])
    term, parts = lax.optimization_barrier((term, parts))
    new_keys, new_values, gates = pl.pallas_call(
        write_kernel,
        out_shape=(cache, cache, jax.ShapeDtypeStruct((SEQS, HEADS, PROPS), F32)),
        in_specs=[vmem()] * 3 + [hbm()] * 4,
        out_specs=(hbm(), hbm(), vmem()),
        scratch_shapes=[
            pltpu.VMEM((2 * SEQS, 2 * PROPS, WIDTH), BF16),
            pltpu.VMEM((2 * SEQS, 2 * PROPS, WIDTH), BF16),
            pltpu.SemaphoreType.DMA((2, 2 * SEQS)),
        ],
        input_output_aliases={5: 0, 6: 1},
        cost_estimate=cost(60_000_000, 1_000_000),
        compiler_params=limit(8),
        name="write",
    )(
        consts, parts, normed, stay(key_cache), stay(value_cache), stay(new_keys), stay(new_values)
    )
    layer_out = (term.astype(F32) + other.astype(F32)).astype(BF16)
    return (layer_out.reshape(SEQS, PROPS, DH), new_keys, new_values, gates.transpose(0, 2, 1))


def solution(mesh):
    placed = (
        P("dp", None, "kv"),
        P("kv"),
        P("kv", "tp"),
        P("kv", "tp"),
        P("kv", "tp"),
        P(),
        P(),
        P(),
        P(),
        P(),
        P("tp", "kv"),
        P("dp", "kv", "tp"),
        P("dp", "kv", "tp"),
        P("dp", "tp", "kv"),
        P("dp"),
        P("dp"),
        P("dp", None),
    )
    return jax.shard_map(
        shards,
        mesh=mesh,
        in_specs=placed,
        out_specs=(
            P("dp", None, "kv"),
            P("dp", "kv", "tp"),
            P("dp", "kv", "tp"),
            P("dp", None, "tp"),
        ),
        check_vma=False,
    )
```
